32 devices in a mesh: sp: 16 (over z, y, x), tp: 2 (over core).
Axes of the slice: x: 2, y: 2, z: 4, core: 2. Of those that a mesh axis runs over, the one named last changes fastest.
Arguments:
- tokens: bfloat16 [4096, 2048], P('sp', 'tp'), may hold values from -6 to 6
- norm_gain: float32 [2, 2048], replicated, may hold values from 0.1 to 1.9
- w_bgate: bfloat16 [2, 2048, 2048], P(None, 'sp', 'tp'), may hold values from -0.125 to 0.125
- w_cgate: bfloat16 [2, 2048, 2048], P(None, 'sp', 'tp'), may hold values from -0.125 to 0.125
- w_value: bfloat16 [2, 2048, 2048], P(None, 'sp', 'tp'), may hold values from -0.125 to 0.125
- conv_taps: float32 [2, 3, 2048], replicated, may hold values from -3.5 to 3.5
- w_out: bfloat16 [2, 2048, 2048], P(None, 'sp', 'tp'), may hold values from -0.125 to 0.125
Outputs:
- mixed_out: bfloat16 [4096, 2048], P('sp', 'tp')
The draws below stay inside these ranges and needn't reach their ends.
All inputs are finite; a program needn't handle non-finite values.
Results may differ from the reference program's by a relative error of at most 0.015.
Values may be sent and summed in bfloat16 or wider, within the bound.
A program may use at most 64 MiB of HBM per device.

```python
import jax
import jax.numpy as jnp
from jax import lax

D = 2048
LAYERS = 2
SEQ = 4096


def steps_of(stream_key, dims, pieces, low, largest):
    gain, own = 1.0, jax.random.fold_in(stream_key, 6)
    for axis_at, blocks in pieces:
        heights = jnp.exp(jax.random.uniform(jax.random.fold_in(own, axis_at), (blocks,), jnp.float32, low / len(pieces), largest / len(pieces)))
        gain = gain * jnp.repeat(heights, dims[axis_at] // blocks).reshape([-1 if axis == axis_at else 1 for axis in range(len(dims))])
    return gain


def bell_draw(stream_key, dims, width, limit, shards=(), kind=jnp.bfloat16):
    loudness = steps_of(stream_key, dims, shards, -0.22, 0.18) if shards else 1.0
    entries = jax.random.normal(stream_key, dims, jnp.float32) * width * loudness
    return jnp.minimum(jnp.maximum(entries, -limit), limit).astype(kind)


def setup_inputs(seed: int = 0) -> dict:
    key_of = jax.random.split(jax.random.key(seed), 8)
    tokens = bell_draw(key_of[0], (SEQ, D), 1.0, 6.0, ((0, 16), (1, 2)))
    norm_gain = jnp.clip(1.0 + 0.18 * jax.random.normal(key_of[1], (LAYERS, D), jnp.float32), 0.1, 1.9)
    w_bgate = bell_draw(key_of[2], (LAYERS, D, D), D ** -0.5, 0.125, ((1, 16), (2, 2)))
    w_cgate = bell_draw(key_of[3], (LAYERS, D, D), D ** -0.5, 0.125, ((1, 16), (2, 2)))
    w_value = bell_draw(key_of[4], (LAYERS, D, D), D ** -0.5, 0.125, ((1, 16), (2, 2)))
    conv_taps = bell_draw(key_of[5], (LAYERS, 3, D), 3 ** -0.5, 3.5, (), jnp.float32)
    w_out = bell_draw(key_of[6], (LAYERS, D, D), D ** -0.5, 0.125, ((1, 16), (2, 2)))
    return {"tokens": tokens, "norm_gain": norm_gain, "w_bgate": w_bgate, "w_cgate": w_cgate, "w_value": w_value, "conv_taps": conv_taps, "w_out": w_out}


def reference(tokens, norm_gain, w_bgate, w_cgate, w_value, conv_taps, w_out):
    current = tokens
    for layer_idx in range(LAYERS):
        as_float = current.astype(jnp.float32)
        scale = lax.rsqrt(lax.optimization_barrier(jnp.mean(as_float * as_float, axis=-1, keepdims=True)) + 1e-06)
        normed = (as_float * scale * norm_gain[layer_idx].astype(jnp.float32)).astype(jnp.bfloat16)
        bgate = lax.optimization_barrier(jnp.dot(normed, w_bgate[layer_idx], preferred_element_type=jnp.float32).astype(jnp.bfloat16))
        cgate = lax.optimization_barrier(jnp.dot(normed, w_cgate[layer_idx], preferred_element_type=jnp.float32).astype(jnp.bfloat16))
        values = lax.optimization_barrier(jnp.dot(normed, w_value[layer_idx], preferred_element_type=jnp.float32).astype(jnp.bfloat16))
        product = cgate.astype(jnp.float32) * values.astype(jnp.float32)
        padded = jnp.pad(product, ((2, 0), (0, 0)))
        taps = conv_taps[layer_idx]
        mixed = taps[0] * padded[:-2] + taps[1] * padded[1:-1] + taps[2] * padded[2:]
        gated = (bgate.astype(jnp.float32) * mixed).astype(jnp.bfloat16)
        update = jnp.dot(gated, w_out[layer_idx], preferred_element_type=jnp.float32)
        current = (as_float + update).astype(jnp.bfloat16)
    return current
```

```python
import functools

import jax
import jax.numpy as jnp
from jax import lax
from jax.experimental import pallas as pl
from jax.experimental.pallas import tpu as pltpu
from jax.sharding import PartitionSpec as P

MESH = pl.DeviceIdType.MESH
LANES = 128
AHEAD = 2
PIECES = 4
F32 = jnp.float32
BF16 = jnp.bfloat16


def mixer_kernel(dims, tok, gain, wb, wc, wv, taps, wo, out,
                 acts, gates, normed, weights, product, cgate, gsend, result, landed,
                 loc_sem, plane_send, plane_recv, line_send, line_recv,
                 ag_send, ag_recv, pair_send, pair_recv,
                 halo_send, halo_recv, out_send, out_recv,
                 tok_send, tok_recv, gate_send, gate_recv,
                 raw, raw_send, raw_recv, guest_send, guest_recv):
    depth, group, line, tps, rows, cols, width, krows = dims
    span = rows * group
    block = krows * group
    tile = span // PIECES
    lend = line >= 4
    guest = depth
    chunks = [(l, m) for l in range(depth) for m in range(4)]
    last = len(chunks)
    sources = (wc, wv, wb, wo)
    sp, t = lax.axis_index("sp"), lax.axis_index("tp")
    z, q = sp // group, sp % group
    own = pl.multiple_of(t * cols + q * width, width)
    end = (z == 0) | (z == line - 1)
    host = (z == 1) | (z == line - 2)
    partner = jnp.where((z == 0) | (z == line - 2), sp + group, sp - group)

    def only(cond, body):
        if lend:
            pl.when(cond)(body)

    def unless_end(body):
        if lend:
            pl.when(jnp.logical_not(end))(body)
        else:
            body()

    def in_plane(d):
        return (z * group + (q + d) % group, t)

    def in_pair(d):
        return (sp, (t + d) % tps)

    def remote(src, dst, send, recv, device):
        return pltpu.make_async_remote_copy(src_ref=src, dst_ref=dst, send_sem=send, recv_sem=recv,
                                            device_id=device, device_id_type=MESH)

    def each(body):
        def step(p, carry):
            body(p)
            return carry

        lax.fori_loop(0, PIECES, step, 0)

    barrier = pltpu.get_barrier_semaphore()

    def hello(device):
        pl.semaphore_signal(barrier, inc=1, device_id=device, device_id_type=MESH)

    for d in range(1, group):
        hello(in_plane(d))
    for d in range(1, tps):
        hello(in_pair(d))

    @pl.when(z > 0)
    def _():
        hello((sp - group, t))

    @pl.when(z < line - 1)
    def _():
        hello((sp + group, t))

    pl.semaphore_wait(barrier, group - 1 + tps - 1
                      + jnp.where(z > 0, 1, 0) + jnp.where(z < line - 1, 1, 0))

    def weight_rows(i, zz, qq):
        l, m = chunks[i]
        return weights.at[l, m, pl.ds(pl.multiple_of((zz * group + qq) * krows, krows), krows), :]

    def weight_block(i, zz):
        l, m = chunks[i]
        return weights.at[l, m, pl.ds(pl.multiple_of(zz * block, block), block), :]

    def weight_source(i, qq):
        l, m = chunks[i]
        return sources[m].at[l, :, pl.ds(pl.multiple_of(qq * width, width), width)]

    def plane_copy(i, d, sender):
        return remote(weight_source(i, (q + d) % group), weight_rows(i, z, sender),
                      plane_send.at[i, d], plane_recv.at[i, d], in_plane(d))

    def local_copy(i):
        return pltpu.make_async_copy(weight_source(i, q), weight_rows(i, z, q), loc_sem.at[i])

    low = 2 * z < line

    def line_copy(i, zz, up):
        blk = weight_block(i, zz)
        return remote(blk, blk, line_send.at[jnp.where(up, 0, 1), i, zz], line_recv.at[i, zz],
                      (jnp.where(up, sp + group, sp - group), t))

    def lent(i):
        l, m = chunks[i]
        return lend and l == 0 and m < 3

    def reach(i):
        return (1, line - 2) if lent(i) else (0, line - 1)

    def goes(i, zz, up):
        lo, hi = reach(i)
        on = jnp.where(up, z < hi, z > lo)
        if lend and not lent(i):
            on = on & jnp.logical_not((zz == z) & (jnp.where(up, z, line - 1 - z) == line - 2))
        return on

    def plane_start(i):
        local_copy(i).start()
        for d in range(1, group):
            plane_copy(i, d, q).start()

    def line_start(i):
        local_copy(i).wait()
        for d in range(1, group):
            plane_copy(i, d, (q + group - d) % group).wait_recv()
        for up in (low, jnp.logical_not(low)):
            @pl.when(goes(i, z, up))
            def _():
                line_copy(i, z, up).start()

    def line_pass(i, up):
        lo, hi = reach(i)

        def step(j, carry):
            zz = jnp.where(up, z - 1 - j, z + 1 + j)
            here = (zz >= 0) & (zz < line) & (z >= lo) & (z <= hi)
            if lend and not lent(i):
                here = here & jnp.logical_not(end & (zz == jnp.where(z == 0, 1, line - 2)))

            @pl.when(here)
            def _():
                line_copy(i, zz, up).wait_recv()

                @pl.when(goes(i, zz, up))
                def _():
                    line_copy(i, zz, up).start()

            return carry

        lax.fori_loop(0, line - 1, step, 0)

    def inward(i):
        line_pass(i, low)

    def outward(i):
        line_pass(i, jnp.logical_not(low))
        if lend and not lent(i):
            @functools.partial(only, end)
            def _():
                for d in range(1, group):
                    guest_copy(i, d, (q + group - d) % group).wait_recv()

    def raw_copy(i, d):
        dst = weight_rows(i, z, q) if d == 0 else raw.at[i, d - 1]
        return remote(weight_source(i, (q + d) % group), dst, raw_send.at[i, d], raw_recv.at[i, d], (partner, t))

    def host_z():
        return jnp.where(z == 0, 1, line - 2)

    def guest_copy(i, d, sender):
        return remote(raw.at[i, d - 1], weight_rows(i, host_z(), sender),
                      guest_send.at[i, d], guest_recv.at[i, d], in_plane(d))

    def raw_take(i):
        for d in range(group):
            if d == 0:
                remote(weight_source(i, q), weight_rows(i, host_z(), q), raw_send.at[i, 0], raw_recv.at[i, 0],
                       (partner, t)).wait_recv()
            else:
                raw_copy(i, d).wait_recv()
                guest_copy(i, d, q).start()

    by_rows = (0, 2 * depth)

    def piece(ph, tt, qq, p, sub=None):
        if ph in by_rows:
            part, slot = rows // PIECES, 0 if ph == 0 else guest
            first, col, wide, buf = qq * rows, tt * cols, cols, acts
        else:
            part, slot = tile, ph // 2
            first, col, wide, buf = 0, tt * cols + qq * width, width, acts if ph % 2 == 0 else gates
        size = part if sub is None else part // 2
        at = first + p * part + (0 if sub is None else sub * size)
        return buf.at[slot, pl.ds(pl.multiple_of(at, size), size), pl.ds(pl.multiple_of(col, wide), wide)]

    def own_piece(ph, p):
        if ph == 0:
            part = rows // PIECES
            return tok.at[pl.ds(pl.multiple_of(p * part, part), part), :]
        return piece(ph, t, q, p)

    def flip(qq, bits):
        if bits & 1:
            qq = qq + 1 - 2 * (qq % 2)
        if bits & 2:
            qq = qq + 2 - 4 * ((qq // 2) % 2)
        return qq

    directs = ([1] if group >= 2 else []) + ([2] if group >= 4 else [])
    relays = [(1, 0, 2), (2, 1, 1)] if group >= 4 else []

    def direct_copy(ph, bits, p, sending):
        return remote(own_piece(ph, p), piece(ph, t, q if sending else flip(q, bits), p),
                      ag_send.at[ph, bits, p], ag_recv.at[ph, bits, p], (z * group + flip(q, bits), t))

    def relay_copy(ph, origin, sub, to, p, sending):
        part = piece(ph, t, flip(q, origin if sending else 3), p, sub)
        return remote(part, part, ag_send.at[ph, 3 + sub, p], ag_recv.at[ph, 3 + sub, p],
                      (z * group + flip(q, to), t))

    def pair_copy(ph, bits, p, d, tt):
        qq = flip(q, bits)
        src = own_piece(ph, p) if bits == 0 else piece(ph, t, qq, p)
        return remote(src, piece(ph, tt, qq, p), pair_send.at[ph, bits, p, d],
                      pair_recv.at[ph, bits, p, d], in_pair(d))

    def pair_start(ph, bits, p):
        for d in range(1, tps):
            pair_copy(ph, bits, p, d, t).start()

    def gather_start(ph, p):
        for bits in directs:
            direct_copy(ph, bits, p, True).start()
        pair_start(ph, 0, p)

    def gather_relay(ph, p):
        for bits in directs:
            direct_copy(ph, bits, p, False).wait_recv()
            for origin, sub, to in relays:
                if origin == bits:
                    relay_copy(ph, origin, sub, to, p, True).start()
            pair_start(ph, bits, p)

    def gather_last(ph, p):
        if relays:
            for origin, sub, to in relays:
                relay_copy(ph, origin, sub, to, p, False).wait_recv()
            pair_start(ph, 3, p)

    def gather_finish(ph, p):
        gather_last(ph, p)
        gather_paired(ph, p)

    def gather_all(ph):
        each(lambda p: gather_last(ph, p))
        each(lambda p: gather_paired(ph, p))

    def gather_paired(ph, p):
        for bits in range(group):
            for d in range(1, tps):
                pair_copy(ph, bits, p, d, (t + tps - d) % tps).wait_recv()

    def gather_sent(ph, p):
        for bits in directs:
            direct_copy(ph, bits, p, True).wait_send()
        for origin, sub, to in relays:
            relay_copy(ph, origin, sub, to, p, True).wait_send()
        for bits in range(group):
            for d in range(1, tps):
                pair_copy(ph, bits, p, d, t).wait_send()

    def token_copy(p):
        return remote(own_piece(0, p), piece(2 * depth, t, q, p), tok_send.at[p], tok_recv.at[p], (partner, t))

    def gate_copy(p):
        return remote(gsend.at[pl.ds(pl.multiple_of(p * tile, tile), tile), :], piece(1, t, q, p),
                      gate_send.at[p], gate_recv.at[p], (partner, t))

    def at_tile(p):
        return pl.ds(pl.multiple_of(p * tile, tile), tile)

    def normalize(slot, l, p):
        sub = min(128, tile)

        def step(i, carry):
            at = pl.ds(pl.multiple_of(p * tile + i * sub, sub), sub)
            x = acts[slot, at, :].astype(F32)
            scale = lax.rsqrt(jnp.mean(x * x, axis=-1, keepdims=True) + 1e-06)
            normed[slot // guest, at, :] = (x * scale * gain[pl.ds(l, 1), :]).astype(BF16)
            return carry

        lax.fori_loop(0, tile // sub, step, 0)

    def project(slot, l, m, p):
        return jnp.dot(normed[slot // guest, at_tile(p), :], weights[l, m], preferred_element_type=F32).astype(BF16)

    def halo_copy(l):
        return remote(product.at[l, pl.ds(span, 8), :], product.at[l, pl.ds(0, 8), :],
                      halo_send.at[l], halo_recv.at[l], (sp + group, t))

    def do_cgate(slot, l, p):
        cgate[at_tile(p), :] = project(slot, l, 0, p)

    def do_values(slot, l, p):
        values = project(slot, l, 1, p)
        product[slot, pl.ds(pl.multiple_of(p * tile + 8, 8), tile), :] = (
            cgate[at_tile(p), :].astype(F32) * values.astype(F32))

    def do_bgate(slot, l, p):
        tap = [taps[l, pl.ds(k, 1), pl.ds(own, width)] for k in range(3)]
        bgate = project(slot, l, 2, p).astype(F32)
        near = product[slot, pl.ds(pl.multiple_of(p * tile, 8), tile + 8), :]
        mixed = tap[0] * near[6:6 + tile] + tap[1] * near[7:7 + tile] + tap[2] * near[8:8 + tile]
        return (bgate * mixed).astype(BF16)

    def no_halo(slot):
        product[slot, pl.ds(0, 8), :] = jnp.zeros((8, width), F32)

    def halo_sender(l):
        return (z >= 1) & (z < line - 2) if lend and l == 0 else z < line - 1

    def halo_taker(l):
        return (z >= 2) & (z < line - 1) if lend and l == 0 else z > 0

    def halo_start(l):
        @pl.when(halo_sender(l))
        def _():
            halo_copy(l).start()

    def halo_ready(l):
        @pl.when(halo_taker(l))
        def _():
            halo_copy(l).wait_recv()

        @pl.when(z == 0)
        def _():
            no_halo(l)

    def do_out(l, p):
        update = jnp.dot(gates[l, at_tile(p), :], weights[l, 3], preferred_element_type=F32)
        return (acts[l, at_tile(p), pl.ds(own, width)].astype(F32) + update).astype(BF16)

    per_owner = rows // tile

    def out_copy(p, sender, owner):
        return remote(result.at[at_tile(p), :],
                      landed.at[pl.ds(pl.multiple_of(p * tile % rows, tile), tile),
                                pl.ds(pl.multiple_of(sender * width, width), width)],
                      out_send.at[p], out_recv.at[sender, p], (z * group + owner, t))

    def own_gate(l, p):
        gates[l, at_tile(p), pl.ds(own, width)] = do_bgate(l, l, p)
        gather_start(2 * l + 1, p)

    guests = 2 * depth
    own_tokens = pltpu.make_async_copy(tok, acts.at[0, pl.ds(pl.multiple_of(q * rows, rows), rows), pl.ds(pl.multiple_of(t * cols, cols), cols)], loc_sem.at[last])
    own_tokens.start()

    @functools.partial(only, end)
    def _():
        each(lambda p: token_copy(p).start())

    rest = range(3, last)

    @functools.partial(only, end)
    def _():
        for i in range(last):
            plane_start(i)
        each(lambda p: gather_start(0, p))
        for i in range(last):
            line_start(i)
            if i in rest:
                raw_take(i)
        own_tokens.wait()
        each(lambda p: gather_relay(0, p))
        gather_all(0)

    @unless_end
    def _():
        for i in range(3):
            plane_start(i)

        @functools.partial(only, host)
        def _():
            for i in rest:
                for d in range(group):
                    raw_copy(i, d).start()

        line_start(0)

        @functools.partial(only, host)
        def _():
            def take(p):
                token_copy(p).wait_recv()
                gather_start(guests, p)
            each(take)

        line_start(1)
        line_start(2)

        @functools.partial(only, host)
        def _():
            gather_relay(guests, 0)
            gather_relay(guests, 1)

        inward(0)

        @functools.partial(only, host)
        def _():
            gather_relay(guests, 2)
            gather_relay(guests, 3)

        each(lambda p: gather_start(0, p))
        plane_start(3)
        inward(1)
        own_tokens.wait()

        @functools.partial(only, host)
        def _():
            gather_all(guests)
            each(lambda p: normalize(guest, 0, p))

        inward(2)
        outward(0)

        @functools.partial(only, host)
        def _():
            each(lambda p: do_cgate(guest, 0, p))

        outward(1)

        @functools.partial(only, host)
        def _():
            each(lambda p: do_values(guest, 0, p))

        each(lambda p: gather_relay(0, p))
        for i in range(4, last):
            plane_start(i)
        inward(3)
        outward(2)

        def lend_gate(p):
            gsend[at_tile(p), :] = do_bgate(guest, 0, p)
            gate_copy(p).start()

        @functools.partial(only, host)
        def _():
            lax.fori_loop(1, PIECES, lambda p, c: (lend_gate(p), c)[1], 0)

        line_start(3)

        gather_all(0)

        def take(p):
            normalize(0, 0, p)
            do_cgate(0, 0, p)
            do_values(0, 0, p)
        each(take)
        halo_start(0)

        @functools.partial(only, host)
        def _():
            @pl.when(z == 1)
            def _():
                no_halo(guest)
                product[0, pl.ds(0, 8), :] = product[guest, pl.ds(span, 8), :]

            @pl.when(z != 1)
            def _():
                product[guest, pl.ds(0, 8), :] = product[0, pl.ds(span, 8), :]

            lend_gate(0)

        inward(4)
        line_start(4)
        outward(3)
        lax.fori_loop(1, PIECES, lambda p, c: (own_gate(0, p), c)[1], 0)
        halo_ready(0)
        own_gate(0, 0)
        for i in range(5, last):
            inward(i)
            line_start(i)

    @functools.partial(only, end)
    def _():
        def take(p):
            gate_copy(p).wait_recv()
            gather_start(1, p)
        take(1)
        take(2)
        gather_relay(1, 1)
        take(3)
        gather_relay(1, 2)
        gather_relay(1, 3)
        take(0)
        outward(3)

    for l in range(depth):
        ph = 2 * l + 1
        if l + 1 < depth:
            def relay_next(k, p):
                on = k < PIECES - 1
                if l == 0 and lend:
                    on = on & (jnp.logical_not(end) | (k == PIECES - 2))

                @pl.when(on)
                def _():
                    gather_relay(ph, (p + 1) % PIECES)

            @unless_end
            def _():
                gather_relay(ph, 1)

            def forward(k):
                p = (k + 1) % PIECES
                relay_next(k, p)

                gather_finish(ph, p)
                acts[l + 1, at_tile(p), pl.ds(own, width)] = do_out(l, p)
                gather_start(ph + 1, p)

                @unless_end
                def _():
                    for n in range(2):
                        @pl.when(k == 2 * n)
                        def _():
                            outward(4 * l + 4 + n)
            each(forward)
            gather_relay(ph + 1, 1)

            def enter(k):
                p = (k + 1) % PIECES

                @pl.when(k < PIECES - 1)
                def _():
                    gather_relay(ph + 1, (p + 1) % PIECES)

                gather_finish(ph + 1, p)
                normalize(l + 1, l + 1, p)

                @unless_end
                def _():
                    @pl.when(k == 1)
                    def _():
                        outward(4 * l + 6)
            each(enter)

            @functools.partial(only, end)
            def _():
                outward(4 * l + 4)
            each(lambda p: do_cgate(l + 1, l + 1, p))

            @functools.partial(only, end)
            def _():
                outward(4 * l + 5)
            each(lambda p: do_values(l + 1, l + 1, p))
            halo_start(l + 1)

            @functools.partial(only, end)
            def _():
                outward(4 * l + 6)

            @unless_end
            def _():
                outward(4 * l + 7)
            lax.fori_loop(1, PIECES, lambda p, c: (own_gate(l + 1, p), c)[1], 0)
            halo_ready(l + 1)
            own_gate(l + 1, 0)
            gather_relay(ph + 2, 1)

            @functools.partial(only, end)
            def _():
                outward(4 * l + 7)
        else:
            def finish(k):
                p = (k + 1) % PIECES

                @pl.when(k < PIECES - 1)
                def _():
                    gather_relay(ph, (p + 1) % PIECES)

                gather_finish(ph, p)
                final = do_out(l, p)
                owner = p * tile // rows

                @pl.when(owner == q)
                def _():
                    landed[pl.ds(pl.multiple_of(p * tile % rows, tile), tile),
                           pl.ds(pl.multiple_of(q * width, width), width)] = final

                @pl.when(owner != q)
                def _():
                    result[at_tile(p), :] = final
                    out_copy(p, q, owner).start()
            each(finish)

    for d in range(1, group):
        for k in range(per_owner):
            out_copy(q * per_owner + k, (q + d) % group, q).wait_recv()
    out[...] = landed[...]

    for i in range(last):
        for d in range(1, group):
            plane_copy(i, d, q).wait_send()

        def step(zz, carry):
            for up in (True, False):
                @pl.when(goes(i, zz, up) & ((zz <= z) if up else (zz >= z)))
                def _():
                    line_copy(i, zz, up).wait_send()

            return carry

        lax.fori_loop(0, line, step, 0)
    for ph in range(2 * depth):
        each(lambda p: gather_sent(ph, p))

    @functools.partial(only, host)
    def _():
        each(lambda p: gather_sent(2 * depth, p))
        each(lambda p: gate_copy(p).wait_send())
        for i in rest:
            for d in range(group):
                raw_copy(i, d).wait_send()

    @functools.partial(only, end)
    def _():
        each(lambda p: token_copy(p).wait_send())
        for i in rest:
            for d in range(1, group):
                guest_copy(i, d, q).wait_send()

    for l in range(depth):
        @pl.when(halo_sender(l))
        def _():
            halo_copy(l).wait_send()

    def sent(p):
        owner = p * tile // rows

        @pl.when(owner != q)
        def _():
            out_copy(p, q, owner).wait_send()
    each(sent)


def shards(sp_size, tps, tokens, norm_gain, w_bgate, w_cgate, w_value, conv_taps, w_out):
    rows, cols = tokens.shape
    depth, krows, _ = w_bgate.shape
    group = 4
    while group > 1 and (sp_size % group or cols % (group * LANES)):
        group //= 2
    line = sp_size // group
    width = cols // group
    span = rows * group
    full = krows * sp_size
    n = 4 * depth
    phases = 2 * depth + 1
    dims = (depth, group, line, tps, rows, cols, width, krows)
    anywhere = pl.BlockSpec(memory_space=pl.ANY)
    vmem = pl.BlockSpec(memory_space=pltpu.VMEM)
    dma = pltpu.SemaphoreType.DMA
    return pl.pallas_call(
        functools.partial(mixer_kernel, dims),
        out_shape=jax.ShapeDtypeStruct((rows, cols), BF16),
        in_specs=[anywhere, vmem, anywhere, anywhere, anywhere, vmem, anywhere],
        out_specs=vmem,
        scratch_shapes=[
            pltpu.VMEM((depth + 1, span, full), BF16),
            pltpu.VMEM((depth, span, full), BF16),
            pltpu.VMEM((2, span, full), BF16),
            pltpu.VMEM((depth, 4, full, width), BF16),
            pltpu.VMEM((depth + 1, span + 8, width), F32),
            pltpu.VMEM((span, width), BF16),
            pltpu.VMEM((span, width), BF16),
            pltpu.VMEM((span, width), BF16),
            pltpu.VMEM((rows, cols), BF16),
            dma((n + 1,)), dma((n, group)), dma((n, group)),
            dma((2, n, line)), dma((n, line)),
            dma((phases, 5, PIECES)), dma((phases, 5, PIECES)),
            dma((phases, group, PIECES, tps)), dma((phases, group, PIECES, tps)),
            dma((depth,)), dma((depth,)), dma((PIECES,)), dma((group, PIECES)),
            dma((PIECES,)), dma((PIECES,)), dma((PIECES,)), dma((PIECES,)),
            pltpu.VMEM((n, group - 1, krows, width), BF16),
            dma((n, group)), dma((n, group)), dma((n, group)), dma((n, group)),
        ],
        compiler_params=pltpu.CompilerParams(
            collective_id=0, has_side_effects=True, vmem_limit_bytes=60 * 1024 * 1024),
    )(tokens, norm_gain, w_bgate, w_cgate, w_value, conv_taps, w_out)


def solution(mesh):
    return jax.shard_map(
        functools.partial(shards, mesh.shape["sp"], mesh.shape["tp"]),
        mesh=mesh,
        in_specs=(
            P("sp", "tp"),
            P(),
            P(None, "sp", "tp"),
            P(None, "sp", "tp"),
            P(None, "sp", "tp"),
            P(),
            P(None, "sp", "tp"),
        ),
        out_specs=P("sp", "tp"),
        check_vma=False,
    )
```

```python
import functools

import jax
import jax.numpy as jnp
from jax import lax
from jax.experimental import pallas as pl
from jax.experimental.pallas import tpu as pltpu
from jax.sharding import PartitionSpec as P

MESH = pl.DeviceIdType.MESH
LANES = 128
AHEAD = 2
PIECES = 4
F32 = jnp.float32
BF16 = jnp.bfloat16


def mixer_kernel(dims, tok, gain, wb, wc, wv, taps, wo, out,
                 acts, gates, normed, weights, product, cgate, gsend, result, landed,
                 loc_sem, plane_send, plane_recv, line_send, line_recv,
                 ag_send, ag_recv, pair_send, pair_recv,
                 halo_send, halo_recv, out_send, out_recv,
                 tok_send, tok_recv, gate_send, gate_recv,
                 raw, raw_send, raw_recv, guest_send, guest_recv):
    depth, group, line, tps, rows, cols, width, krows = dims
    span = rows * group
    block = krows * group
    tile = span // PIECES
    lend = line >= 4
    guest = depth
    chunks = [(l, m) for l in range(depth) for m in range(4)]
    last = len(chunks)
    sources = (wc, wv, wb, wo)
    sp, t = lax.axis_index("sp"), lax.axis_index("tp")
    z, q = sp // group, sp % group
    own = pl.multiple_of(t * cols + q * width, width)
    end = (z == 0) | (z == line - 1)
    host = (z == 1) | (z == line - 2)
    partner = jnp.where((z == 0) | (z == line - 2), sp + group, sp - group)

    def only(cond, body):
        if lend:
            pl.when(cond)(body)

    def unless_end(body):
        if lend:
            pl.when(jnp.logical_not(end))(body)
        else:
            body()

    def in_plane(d):
        return (z * group + (q + d) % group, t)

    def in_pair(d):
        return (sp, (t + d) % tps)

    def remote(src, dst, send, recv, device):
        return pltpu.make_async_remote_copy(src_ref=src, dst_ref=dst, send_sem=send, recv_sem=recv,
                                            device_id=device, device_id_type=MESH)

    def each(body):
        def step(p, carry):
            body(p)
            return carry

        lax.fori_loop(0, PIECES, step, 0)

    barrier = pltpu.get_barrier_semaphore()

    def hello(device):
        pl.semaphore_signal(barrier, inc=1, device_id=device, device_id_type=MESH)

    for d in range(1, group):
        hello(in_plane(d))
    for d in range(1, tps):
        hello(in_pair(d))

    @pl.when(z > 0)
    def _():
        hello((sp - group, t))

    @pl.when(z < line - 1)
    def _():
        hello((sp + group, t))

    pl.semaphore_wait(barrier, group - 1 + tps - 1
                      + jnp.where(z > 0, 1, 0) + jnp.where(z < line - 1, 1, 0))

    def weight_rows(i, zz, qq):
        l, m = chunks[i]
        return weights.at[l, m, pl.ds(pl.multiple_of((zz * group + qq) * krows, krows), krows), :]

    def weight_block(i, zz):
        l, m = chunks[i]
        return weights.at[l, m, pl.ds(pl.multiple_of(zz * block, block), block), :]

    def weight_source(i, qq):
        l, m = chunks[i]
        return sources[m].at[l, :, pl.ds(pl.multiple_of(qq * width, width), width)]

    def plane_copy(i, d, sender):
        return remote(weight_source(i, (q + d) % group), weight_rows(i, z, sender),
                      plane_send, plane_recv.at[i], in_plane(d))

    def local_copy(i):
        return pltpu.make_async_copy(weight_source(i, q), weight_rows(i, z, q), loc_sem.at[i])

    low = 2 * z < line

    def share(i):
        l, m = chunks[i]
        return l if l == 0 and m < 3 else l + 1 if l else 1

    def line_copy(i, zz, up):
        blk = weight_block(i, zz)
        return remote(blk, blk, line_send.at[jnp.where(up, 0, 1), share(i), zz], line_recv.at[i, zz],
                      (jnp.where(up, sp + group, sp - group), t))

    def lent(i):
        l, m = chunks[i]
        return lend and l == 0 and m < 3

    def reach(i):
        return (1, line - 2) if lent(i) else (0, line - 1)

    def goes(i, zz, up):
        lo, hi = reach(i)
        on = jnp.where(up, z < hi, z > lo)
        if lend and not lent(i):
            on = on & jnp.logical_not((zz == z) & (jnp.where(up, z, line - 1 - z) == line - 2))
        return on

    def plane_start(i):
        local_copy(i).start()
        for d in range(1, group):
            plane_copy(i, d, q).start()

    def line_start(i):
        local_copy(i).wait()
        if group > 1:
            ref = some_rows(i, group - 1)
            remote(ref, ref, plane_send, plane_recv.at[i], in_plane(1)).wait_recv()
        for up in (low, jnp.logical_not(low)):
            @pl.when(goes(i, z, up))
            def _():
                line_copy(i, z, up).start()

    def line_pass(i, up):
        lo, hi = reach(i)

        def step(j, carry):
            zz = jnp.where(up, z - 1 - j, z + 1 + j)
            here = (zz >= 0) & (zz < line) & (z >= lo) & (z <= hi)
            if lend and not lent(i):
                here = here & jnp.logical_not(end & (zz == jnp.where(z == 0, 1, line - 2)))

            @pl.when(here)
            def _():
                line_copy(i, zz, up).wait_recv()

                @pl.when(goes(i, zz, up))
                def _():
                    line_copy(i, zz, up).start()

            return carry

        lax.fori_loop(0, line - 1, step, 0)

    def inward(i):
        line_pass(i, low)

    def outward(i):
        line_pass(i, jnp.logical_not(low))
        if lend and not lent(i):
            @functools.partial(only, end)
            def _():
                if group > 1:
                    ref = some_rows(i, group - 1)
                    remote(ref, ref, guest_send.at[i], guest_recv.at[i], in_plane(1)).wait_recv()

    def raw_copy(i, d):
        dst = weight_rows(i, z, q) if d == 0 else raw.at[i, d - 1]
        return remote(weight_source(i, (q + d) % group), dst, raw_send.at[i], raw_recv.at[i], (partner, t))

    def host_z():
        return jnp.where(z == 0, 1, line - 2)

    def guest_copy(i, d, sender):
        return remote(raw.at[i, d - 1], weight_rows(i, host_z(), sender),
                      guest_send.at[i], guest_recv.at[i], in_plane(d))

    def raw_take(i):
        ref = some_rows(i, group)
        remote(ref, ref, raw_send.at[i], raw_recv.at[i], (partner, t)).wait_recv()
        for d in range(1, group):
            guest_copy(i, d, q).start()

    by_rows = (0, 2 * depth)

    def piece(ph, tt, qq, p, sub=None):
        if ph in by_rows:
            part, slot = rows // PIECES, 0 if ph == 0 else guest
            first, col, wide, buf = qq * rows, tt * cols, cols, acts
        else:
            part, slot = tile, ph // 2
            first, col, wide, buf = 0, tt * cols + qq * width, width, acts if ph % 2 == 0 else gates
        size = part if sub is None else part // 2
        at = first + p * part + (0 if sub is None else sub * size)
        return buf.at[slot, pl.ds(pl.multiple_of(at, size), size), pl.ds(pl.multiple_of(col, wide), wide)]

    def own_piece(ph, p):
        if ph == 0:
            part = rows // PIECES
            return tok.at[pl.ds(pl.multiple_of(p * part, part), part), :]
        return piece(ph, t, q, p)

    def flip(qq, bits):
        if bits & 1:
            qq = qq + 1 - 2 * (qq % 2)
        if bits & 2:
            qq = qq + 2 - 4 * ((qq // 2) % 2)
        return qq

    directs = ([1] if group >= 2 else []) + ([2] if group >= 4 else [])
    relays = [(1, 0, 2), (2, 1, 1)] if group >= 4 else []

    def direct_copy(ph, bits, p, sending):
        return remote(own_piece(ph, p), piece(ph, t, q if sending else flip(q, bits), p),
                      ag_send.at[ph], ag_recv.at[ph, bits - 1, p], (z * group + flip(q, bits), t))

    def relay_copy(ph, origin, sub, to, p, sending):
        part = piece(ph, t, flip(q, origin if sending else 3), p, sub)
        return remote(part, part, ag_send.at[ph], ag_recv.at[ph, 2, p],
                      (z * group + flip(q, to), t))

    def pair_copy(ph, bits, p, d, tt):
        qq = flip(q, bits)
        src = own_piece(ph, p) if bits == 0 else piece(ph, t, qq, p)
        return remote(src, piece(ph, tt, qq, p), pair_send.at[ph, d - 1],
                      pair_recv.at[ph, p, d - 1], in_pair(d))

    def pair_start(ph, bits, p):
        for d in range(1, tps):
            pair_copy(ph, bits, p, d, t).start()

    def gather_start(ph, p):
        for bits in directs:
            direct_copy(ph, bits, p, True).start()
        pair_start(ph, 0, p)

    def gather_relay(ph, p):
        for bits in directs:
            direct_copy(ph, bits, p, False).wait_recv()
            for origin, sub, to in relays:
                if origin == bits:
                    relay_copy(ph, origin, sub, to, p, True).start()
            pair_start(ph, bits, p)

    def gather_last(ph, p):
        if relays:
            part = piece(ph, t, flip(q, 3), p)
            remote(part, part, ag_send.at[ph], ag_recv.at[ph, 2, p], in_plane(1)).wait_recv()
            pair_start(ph, 3, p)

    def gather_finish(ph, p):
        gather_last(ph, p)
        gather_paired(ph, p)

    def gather_all(ph):
        each(lambda p: gather_last(ph, p))
        each(lambda p: gather_paired(ph, p))

    def gather_paired(ph, p):
        for d in range(1, tps):
            if ph in by_rows:
                ref = acts.at[0, pl.ds(0, span // PIECES), pl.ds(0, cols)]
            else:
                ref = acts.at[0, pl.ds(0, tile), pl.ds(0, cols)]
            remote(ref, ref, pair_send.at[ph, d - 1], pair_recv.at[ph, p, d - 1], in_pair(d)).wait_recv()

    def all_sent(ref, sem):
        remote(ref, ref, sem, sem, in_pair(1)).wait_send()

    def gather_sent(ph):
        k = len(directs) + len(relays) // 2
        if k:
            all_sent(acts.at[0, pl.ds(0, k * rows), pl.ds(0, cols)] if ph in by_rows
                     else acts.at[0, pl.ds(0, span), pl.ds(0, k * width)], ag_send.at[ph])
        for d in range(1, tps):
            all_sent(acts.at[0, pl.ds(0, span), pl.ds(0, cols)], pair_send.at[ph, d - 1])

    def plane_sent():
        if group > 1:
            all_sent(weights.at[:, :, pl.ds(0, (group - 1) * krows), :], plane_send)

    def some_rows(i, pieces):
        l, m = chunks[i]
        return weights.at[l, m, pl.ds(0, pieces * krows), :]

    def line_sent(batch):
        l, m = chunks[batch[0]]
        ref = weights.at[l, pl.ds(m, len(batch)), pl.ds(0, block), :]

        def step(zz, carry):
            for up in (True, False):
                @pl.when(goes(batch[0], zz, up) & ((zz <= z) if up else (zz >= z)))
                def _():
                    all_sent(ref, line_send.at[0 if up else 1, share(batch[0]), zz])

            return carry

        lax.fori_loop(0, line, step, 0)

    def early_sent():
        plane_sent()
        gather_sent(0)
        gather_sent(1)
        line_sent(range(3))
        line_sent(range(3, 4))

        @functools.partial(only, host)
        def _():
            gather_sent(guests)
            all_sent(gsend, gate_send)
            for i in rest:
                all_sent(some_rows(i, group), raw_send.at[i])

        @functools.partial(only, end)
        def _():
            all_sent(acts.at[0, pl.ds(0, rows), pl.ds(0, cols)], tok_send)
            for i in rest:
                if group > 1:
                    all_sent(some_rows(i, group - 1), guest_send.at[i])

    def token_copy(p):
        return remote(own_piece(0, p), piece(2 * depth, t, q, p), tok_send, tok_recv.at[p], (partner, t))

    def gate_copy(p):
        return remote(gsend.at[pl.ds(pl.multiple_of(p * tile, tile), tile), :], piece(1, t, q, p),
                      gate_send, gate_recv.at[p], (partner, t))

    def at_tile(p):
        return pl.ds(pl.multiple_of(p * tile, tile), tile)

    def normalize(slot, l, p):
        sub = min(128, tile)

        def step(i, carry):
            at = pl.ds(pl.multiple_of(p * tile + i * sub, sub), sub)
            x = acts[slot, at, :].astype(F32)
            scale = lax.rsqrt(jnp.mean(x * x, axis=-1, keepdims=True) + 1e-06)
            normed[slot // guest, at, :] = (x * scale * gain[pl.ds(l, 1), :]).astype(BF16)
            return carry

        lax.fori_loop(0, tile // sub, step, 0)

    def project(slot, l, m, p):
        return jnp.dot(normed[slot // guest, at_tile(p), :], weights[l, m], preferred_element_type=F32).astype(BF16)

    def halo_copy(l):
        return remote(product.at[l, pl.ds(span, 8), :], product.at[l, pl.ds(0, 8), :],
                      halo_send.at[l], halo_recv.at[l], (sp + group, t))

    def do_cgate(slot, l, p):
        cgate[at_tile(p), :] = project(slot, l, 0, p)

    def do_values(slot, l, p):
        values = project(slot, l, 1, p)
        product[slot, pl.ds(pl.multiple_of(p * tile + 8, 8), tile), :] = (
            cgate[at_tile(p), :].astype(F32) * values.astype(F32))

    def do_bgate(slot, l, p):
        tap = [taps[k, pl.ds(l, 1), pl.ds(own, width)] for k in range(3)]
        bgate = project(slot, l, 2, p).astype(F32)
        near = product[slot, pl.ds(pl.multiple_of(p * tile, 8), tile + 8), :]
        mixed = tap[0] * near[6:6 + tile] + tap[1] * near[7:7 + tile] + tap[2] * near[8:8 + tile]
        return (bgate * mixed).astype(BF16)

    def no_halo(slot):
        product[slot, pl.ds(0, 8), :] = jnp.zeros((8, width), F32)

    def halo_sender(l):
        return (z >= 1) & (z < line - 2) if lend and l == 0 else z < line - 1

    def halo_taker(l):
        return (z >= 2) & (z < line - 1) if lend and l == 0 else z > 0

    def halo_start(l):
        @pl.when(halo_sender(l))
        def _():
            halo_copy(l).start()

    def halo_ready(l):
        @pl.when(halo_taker(l))
        def _():
            halo_copy(l).wait_recv()

        @pl.when(z == 0)
        def _():
            no_halo(l)

    def do_out(l, p):
        update = jnp.dot(gates[l, at_tile(p), :], weights[l, 3], preferred_element_type=F32)
        return (acts[l, at_tile(p), pl.ds(own, width)].astype(F32) + update).astype(BF16)

    per_owner = rows // tile

    def out_copy(p, sender, owner):
        return remote(result.at[at_tile(p), :],
                      landed.at[pl.ds(pl.multiple_of(p * tile % rows, tile), tile),
                                pl.ds(pl.multiple_of(sender * width, width), width)],
                      out_send, out_recv, (z * group + owner, t))

    def own_gate(l, p):
        gates[l, at_tile(p), pl.ds(own, width)] = do_bgate(l, l, p)
        gather_start(2 * l + 1, p)

    guests = 2 * depth
    own_tokens = pltpu.make_async_copy(tok, acts.at[0, pl.ds(pl.multiple_of(q * rows, rows), rows), pl.ds(pl.multiple_of(t * cols, cols), cols)], loc_sem.at[last])
    own_tokens.start()

    @functools.partial(only, end)
    def _():
        each(lambda p: token_copy(p).start())

    rest = range(3, last)

    @functools.partial(only, end)
    def _():
        for i in range(last):
            plane_start(i)
        each(lambda p: gather_start(0, p))
        for i in range(last):
            line_start(i)
            if i in rest:
                raw_take(i)
        own_tokens.wait()
        each(lambda p: gather_relay(0, p))
        gather_all(0)

    @unless_end
    def _():
        for i in range(3):
            plane_start(i)

        @functools.partial(only, host)
        def _():
            for i in rest:
                for d in range(group):
                    raw_copy(i, d).start()

        line_start(0)

        @functools.partial(only, host)
        def _():
            def take(p):
                token_copy(p).wait_recv()
                gather_start(guests, p)
            each(take)

        line_start(1)
        line_start(2)

        @functools.partial(only, host)
        def _():
            gather_relay(guests, 0)
            gather_relay(guests, 1)

        inward(0)

        @functools.partial(only, host)
        def _():
            gather_relay(guests, 2)
            gather_relay(guests, 3)

        each(lambda p: gather_start(0, p))
        plane_start(3)
        inward(1)
        own_tokens.wait()

        @functools.partial(only, host)
        def _():
            gather_all(guests)
            each(lambda p: normalize(guest, 0, p))

        inward(2)
        outward(0)

        @functools.partial(only, host)
        def _():
            each(lambda p: do_cgate(guest, 0, p))

        outward(1)

        @functools.partial(only, host)
        def _():
            each(lambda p: do_values(guest, 0, p))

        each(lambda p: gather_relay(0, p))
        for i in range(4, last):
            plane_start(i)
        inward(3)
        outward(2)

        def lend_gate(p):
            gsend[at_tile(p), :] = do_bgate(guest, 0, p)
            gate_copy(p).start()

        @functools.partial(only, host)
        def _():
            lax.fori_loop(1, PIECES, lambda p, c: (lend_gate(p), c)[1], 0)

        line_start(3)
        inward(4)

        each(lambda p: gather_last(0, p))
        outward(3)
        line_start(4)
        inward(5)
        each(lambda p: gather_paired(0, p))

        def take(p):
            normalize(0, 0, p)
            do_cgate(0, 0, p)
            do_values(0, 0, p)
        each(take)
        halo_start(0)

        @functools.partial(only, host)
        def _():
            @pl.when(z == 1)
            def _():
                no_halo(guest)
                product[0, pl.ds(0, 8), :] = product[guest, pl.ds(span, 8), :]

            @pl.when(z != 1)
            def _():
                product[guest, pl.ds(0, 8), :] = product[0, pl.ds(span, 8), :]

            lend_gate(0)

        line_start(5)
        lax.fori_loop(1, PIECES, lambda p, c: (own_gate(0, p), c)[1], 0)
        halo_ready(0)
        own_gate(0, 0)
        for i in range(6, last):
            inward(i)
            line_start(i)

    @functools.partial(only, end)
    def _():
        def take(p):
            gate_copy(p).wait_recv()
            gather_start(1, p)
        take(1)
        take(2)
        gather_relay(1, 1)
        take(3)
        gather_relay(1, 2)
        gather_relay(1, 3)
        take(0)
        outward(3)

    for l in range(depth):
        ph = 2 * l + 1
        if l + 1 < depth:
            def relay_next(k, p):
                on = k < PIECES - 1
                if l == 0 and lend:
                    on = on & (jnp.logical_not(end) | (k == PIECES - 2))

                @pl.when(on)
                def _():
                    gather_relay(ph, (p + 1) % PIECES)

            @unless_end
            def _():
                gather_relay(ph, 1)

            def forward(k):
                p = (k + 1) % PIECES
                relay_next(k, p)

                @unless_end
                def _():
                    for n in range(2):
                        @pl.when(k == (0, PIECES - 1)[n])
                        def _():
                            outward(4 * l + 4 + n)

                gather_finish(ph, p)
                acts[l + 1, at_tile(p), pl.ds(own, width)] = do_out(l, p)
                gather_start(ph + 1, p)
            each(forward)
            @unless_end
            def _():
                outward(4 * l + 6)
            each(lambda k: gather_relay(ph + 1, (k + 1) % PIECES))

            @functools.partial(only, end)
            def _():
                outward(4 * l + 4)
                outward(4 * l + 5)

            early_sent()

            def enter(p):
                gather_paired(ph + 1, p)
                normalize(l + 1, l + 1, p)
                do_cgate(l + 1, l + 1, p)
                do_values(l + 1, l + 1, p)

            gather_last(ph + 1, 1)
            gather_last(ph + 1, 2)
            enter(1)
            gather_last(ph + 1, 3)
            enter(2)

            @functools.partial(only, end)
            def _():
                outward(4 * l + 6)
            own_gate(l + 1, 2)
            gather_last(ph + 1, 0)
            enter(3)
            halo_start(l + 1)
            own_gate(l + 1, 3)

            @unless_end
            def _():
                outward(4 * l + 7)
            enter(0)
            own_gate(l + 1, 1)
            halo_ready(l + 1)
            own_gate(l + 1, 0)
            gather_relay(ph + 2, 2)

            @functools.partial(only, end)
            def _():
                outward(4 * l + 7)
        else:
            def finish(k):
                p = jnp.where(k < 2, k + 2, 3 - k)

                @pl.when(k < PIECES - 1)
                def _():
                    gather_relay(ph, jnp.where(k < 1, 3, 2 - k))

                gather_finish(ph, p)
                final = do_out(l, p)
                owner = p * tile // rows

                @pl.when(owner == q)
                def _():
                    landed[pl.ds(pl.multiple_of(p * tile % rows, tile), tile),
                           pl.ds(pl.multiple_of(q * width, width), width)] = final

                @pl.when(owner != q)
                def _():
                    result[at_tile(p), :] = final
                    out_copy(p, q, owner).start()
            each(finish)

    if group > 1:
        ref = landed.at[:, pl.ds(0, (group - 1) * width)]
        remote(ref, ref, out_send, out_recv, in_plane(1)).wait_recv()
    out[...] = landed[...]

    for l in range(1, depth):
        line_sent(range(4 * l, 4 * l + 4))
    for ph in range(2, 2 * depth):
        gather_sent(ph)

    for l in range(depth):
        @pl.when(halo_sender(l))
        def _():
            halo_copy(l).wait_send()

    if group > 1:
        all_sent(result.at[pl.ds(0, (PIECES - per_owner) * tile), :], out_send)


def shards(sp_size, tps, tokens, norm_gain, w_bgate, w_cgate, w_value, conv_taps, w_out):
    rows, cols = tokens.shape
    depth, krows, _ = w_bgate.shape
    group = 4
    while group > 1 and (sp_size % group or cols % (group * LANES)):
        group //= 2
    line = sp_size // group
    width = cols // group
    span = rows * group
    full = krows * sp_size
    n = 4 * depth
    phases = 2 * depth + 1
    others = max(1, tps - 1)
    dims = (depth, group, line, tps, rows, cols, width, krows)
    anywhere = pl.BlockSpec(memory_space=pl.ANY)
    vmem = pl.BlockSpec(memory_space=pltpu.VMEM)
    dma = pltpu.SemaphoreType.DMA
    return pl.pallas_call(
        functools.partial(mixer_kernel, dims),
        out_shape=jax.ShapeDtypeStruct((rows, cols), BF16),
        in_specs=[anywhere, vmem, anywhere, anywhere, anywhere, vmem, anywhere],
        out_specs=vmem,
        scratch_shapes=[
            pltpu.VMEM((depth + 1, span, full), BF16),
            pltpu.VMEM((depth, span, full), BF16),
            pltpu.VMEM((2, span, full), BF16),
            pltpu.VMEM((depth, 4, full, width), BF16),
            pltpu.VMEM((depth + 1, span + 8, width), F32),
            pltpu.VMEM((span, width), BF16),
            pltpu.VMEM((span, width), BF16),
            pltpu.VMEM((span, width), BF16),
            pltpu.VMEM((rows, cols), BF16),
            dma((n + 1,)), dma(()), dma((n,)),
            dma((2, depth + 1, line)), dma((n, line)),
            dma((phases,)), dma((phases, 3, PIECES)),
            dma((phases, others)), dma((phases, PIECES, others)),
            dma((depth,)), dma((depth,)), dma(()), dma(()),
            dma(()), dma((PIECES,)), dma(()), dma((PIECES,)),
            pltpu.VMEM((n, max(1, group - 1), krows, width), BF16),
            dma((n,)), dma((n,)), dma((n,)), dma((n,)),
        ],
        compiler_params=pltpu.CompilerParams(
            collective_id=0, has_side_effects=True, vmem_limit_bytes=60 * 1024 * 1024),
    )(tokens, norm_gain, w_bgate, w_cgate, w_value, conv_taps.transpose(1, 0, 2), w_out)


def solution(mesh):
    return jax.shard_map(
        functools.partial(shards, mesh.shape["sp"], mesh.shape["tp"]),
        mesh=mesh,
        in_specs=(
            P("sp", "tp"),
            P(),
            P(None, "sp", "tp"),
            P(None, "sp", "tp"),
            P(None, "sp", "tp"),
            P(),
            P(None, "sp", "tp"),
        ),
        out_specs=P("sp", "tp"),
        check_vma=False,
    )
```

```python
import functools

import jax
import jax.numpy as jnp
from jax import lax
from jax.experimental import pallas as pl
from jax.experimental.pallas import tpu as pltpu
from jax.sharding import PartitionSpec as P

MESH = pl.DeviceIdType.MESH
LANES = 128
AHEAD = 2
PIECES = 4
F32 = jnp.float32
BF16 = jnp.bfloat16


def mixer_kernel(dims, tok, gain, wb, wc, wv, taps, wo, out,
                 acts, gates, normed, weights, product, cgate, gsend, result, landed,
                 loc_sem, plane_send, plane_recv, line_send, line_recv,
                 ag_send, ag_recv, pair_send, pair_recv,
                 halo_send, halo_recv, out_send, out_recv,
                 tok_send, tok_recv, gate_send, gate_recv,
                 raw, raw_send, raw_recv, guest_send, guest_recv):
    depth, group, line, tps, rows, cols, width, krows = dims
    span = rows * group
    block = krows * group
    tile = span // PIECES
    part = rows // PIECES
    lend = line >= 4
    guest = depth
    chunks = [(l, m) for l in range(depth) for m in range(4)]
    last = len(chunks)
    sources = (wc, wv, wb, wo)
    sp, t = lax.axis_index("sp"), lax.axis_index("tp")
    z, q = sp // group, sp % group
    own = pl.multiple_of(t * cols + q * width, width)
    end = (z == 0) | (z == line - 1)
    host = (z == 1) | (z == line - 2)
    partner = jnp.where((z == 0) | (z == line - 2), sp + group, sp - group)

    def only(cond, body):
        if lend:
            pl.when(cond)(body)

    def unless_end(body):
        if lend:
            pl.when(jnp.logical_not(end))(body)
        else:
            body()

    def in_plane(d):
        return (z * group + (q + d) % group, t)

    def in_pair(d):
        return (sp, (t + d) % tps)

    def remote(src, dst, send, recv, device):
        return pltpu.make_async_remote_copy(src_ref=src, dst_ref=dst, send_sem=send, recv_sem=recv,
                                            device_id=device, device_id_type=MESH)

    def each(body):
        def step(p, carry):
            body(p)
            return carry

        lax.fori_loop(0, PIECES, step, 0)

    barrier = pltpu.get_barrier_semaphore()

    def hello(device):
        pl.semaphore_signal(barrier, inc=1, device_id=device, device_id_type=MESH)

    for d in range(1, group):
        hello(in_plane(d))
    for d in range(1, tps):
        hello(in_pair(d))

    @pl.when(z > 0)
    def _():
        hello((sp - group, t))

    @pl.when(z < line - 1)
    def _():
        hello((sp + group, t))

    pl.semaphore_wait(barrier, group - 1 + tps - 1
                      + jnp.where(z > 0, 1, 0) + jnp.where(z < line - 1, 1, 0))

    def weight_rows(i, zz, qq):
        l, m = chunks[i]
        return weights.at[l, m, pl.ds(pl.multiple_of((zz * group + qq) * krows, krows), krows), :]

    def weight_block(i, zz):
        l, m = chunks[i]
        return weights.at[l, m, pl.ds(pl.multiple_of(zz * block, block), block), :]

    def weight_source(i, qq):
        l, m = chunks[i]
        return sources[m].at[l, :, pl.ds(pl.multiple_of(qq * width, width), width)]

    def plane_copy(i, d, sender):
        return remote(weight_source(i, (q + d) % group), weight_rows(i, z, sender),
                      plane_send, plane_recv.at[i], in_plane(d))

    def local_copy(i):
        return pltpu.make_async_copy(weight_source(i, q), weight_rows(i, z, q), loc_sem.at[i])

    low = 2 * z < line

    def share(i):
        l, m = chunks[i]
        return l if l == 0 and m < 3 else l + 1 if l else 1

    def line_copy(i, zz, up):
        blk = weight_block(i, zz)
        return remote(blk, blk, line_send.at[jnp.where(up, 0, 1), share(i), zz], line_recv.at[i, zz],
                      (jnp.where(up, sp + group, sp - group), t))

    def lent(i):
        l, m = chunks[i]
        return lend and l == 0 and m < 3

    def reach(i):
        return (1, line - 2) if lent(i) else (0, line - 1)

    def goes(i, zz, up):
        lo, hi = reach(i)
        on = jnp.where(up, z < hi, z > lo)
        if lend and not lent(i):
            on = on & jnp.logical_not((zz == z) & (jnp.where(up, z, line - 1 - z) == line - 2))
        return on

    def plane_start(i):
        local_copy(i).start()
        for d in range(1, group):
            plane_copy(i, d, q).start()

    def line_start(i):
        local_copy(i).wait()
        if group > 1:
            ref = some_rows(i, group - 1)
            remote(ref, ref, plane_send, plane_recv.at[i], in_plane(1)).wait_recv()
        for up in (low, jnp.logical_not(low)):
            @pl.when(goes(i, z, up))
            def _():
                line_copy(i, z, up).start()

    def line_pass(i, up):
        lo, hi = reach(i)

        def step(j, carry):
            zz = jnp.where(up, z - 1 - j, z + 1 + j)
            here = (zz >= 0) & (zz < line) & (z >= lo) & (z <= hi)
            if lend and not lent(i):
                here = here & jnp.logical_not(end & (zz == jnp.where(z == 0, 1, line - 2)))

            @pl.when(here)
            def _():
                line_copy(i, zz, up).wait_recv()

                @pl.when(goes(i, zz, up))
                def _():
                    line_copy(i, zz, up).start()

            return carry

        lax.fori_loop(0, line - 1, step, 0)

    def inward(i):
        line_pass(i, low)

    def outward(i):
        line_pass(i, jnp.logical_not(low))
        if lend and not lent(i):
            @functools.partial(only, end)
            def _():
                if group > 1:
                    ref = some_rows(i, group - 1)
                    remote(ref, ref, guest_send.at[i], guest_recv.at[i], in_plane(1)).wait_recv()

    def raw_copy(i, d):
        dst = weight_rows(i, z, q) if d == 0 else raw.at[i, d - 1]
        return remote(weight_source(i, (q + d) % group), dst, raw_send.at[i], raw_recv.at[i], (partner, t))

    def host_z():
        return jnp.where(z == 0, 1, line - 2)

    def guest_copy(i, d, sender):
        return remote(raw.at[i, d - 1], weight_rows(i, host_z(), sender),
                      guest_send.at[i], guest_recv.at[i], in_plane(d))

    def raw_take(i):
        ref = some_rows(i, group)
        remote(ref, ref, raw_send.at[i], raw_recv.at[i], (partner, t)).wait_recv()
        for d in range(1, group):
            guest_copy(i, d, q).start()

    by_rows = (0, 2 * depth)

    def piece(ph, tt, qq, p, sub=None):
        if ph in by_rows:
            size, slot, at = part, 0 if ph == 0 else guest, p * tile + qq * part
            col, wide, buf = tt * cols, cols, acts
        else:
            size, slot, at = tile, ph // 2, p * tile
            col, wide, buf = tt * cols + qq * width, width, acts if ph % 2 == 0 else gates
        if sub is not None:
            size = size // 2
            at = at + sub * size
        return buf.at[slot, pl.ds(pl.multiple_of(at, size), size), pl.ds(pl.multiple_of(col, wide), wide)]

    def own_piece(ph, p):
        if ph == 0:
            return tok.at[pl.ds(pl.multiple_of(p * part, part), part), :]
        return piece(ph, t, q, p)

    def flip(qq, bits):
        if bits & 1:
            qq = qq + 1 - 2 * (qq % 2)
        if bits & 2:
            qq = qq + 2 - 4 * ((qq // 2) % 2)
        return qq

    directs = ([1] if group >= 2 else []) + ([2] if group >= 4 else [])
    relays = [(1, 0, 2), (2, 1, 1)] if group >= 4 else []

    def direct_copy(ph, bits, p, sending):
        return remote(own_piece(ph, p), piece(ph, t, q if sending else flip(q, bits), p),
                      ag_send.at[ph], ag_recv.at[ph, bits - 1, p], (z * group + flip(q, bits), t))

    def relay_copy(ph, origin, sub, to, p, sending):
        ref = piece(ph, t, flip(q, origin if sending else 3), p, sub)
        return remote(ref, ref, ag_send.at[ph], ag_recv.at[ph, 2, p],
                      (z * group + flip(q, to), t))

    def pair_copy(ph, bits, p, d, tt):
        qq = flip(q, bits)
        src = own_piece(ph, p) if bits == 0 else piece(ph, t, qq, p)
        return remote(src, piece(ph, tt, qq, p), pair_send.at[ph, d - 1],
                      pair_recv.at[ph, p, d - 1], in_pair(d))

    def pair_start(ph, bits, p):
        for d in range(1, tps):
            pair_copy(ph, bits, p, d, t).start()

    def gather_start(ph, p):
        for bits in directs:
            direct_copy(ph, bits, p, True).start()
        pair_start(ph, 0, p)

    def gather_relay(ph, p):
        for bits in directs:
            direct_copy(ph, bits, p, False).wait_recv()
            for origin, sub, to in relays:
                if origin == bits:
                    relay_copy(ph, origin, sub, to, p, True).start()
            pair_start(ph, bits, p)

    def gather_last(ph, p):
        if relays:
            ref = piece(ph, t, flip(q, 3), p)
            remote(ref, ref, ag_send.at[ph], ag_recv.at[ph, 2, p], in_plane(1)).wait_recv()
            pair_start(ph, 3, p)

    def gather_finish(ph, p):
        gather_last(ph, p)
        gather_paired(ph, p)

    def gather_all(ph):
        each(lambda p: gather_last(ph, p))
        each(lambda p: gather_paired(ph, p))

    def gather_paired(ph, p):
        for d in range(1, tps):
            if ph in by_rows:
                ref = acts.at[0, pl.ds(0, span // PIECES), pl.ds(0, cols)]
            else:
                ref = acts.at[0, pl.ds(0, tile), pl.ds(0, cols)]
            remote(ref, ref, pair_send.at[ph, d - 1], pair_recv.at[ph, p, d - 1], in_pair(d)).wait_recv()

    def all_sent(ref, sem):
        remote(ref, ref, sem, sem, in_pair(1)).wait_send()

    def gather_sent(ph):
        k = len(directs) + len(relays) // 2
        if k:
            all_sent(acts.at[0, pl.ds(0, k * rows), pl.ds(0, cols)] if ph in by_rows
                     else acts.at[0, pl.ds(0, span), pl.ds(0, k * width)], ag_send.at[ph])
        for d in range(1, tps):
            all_sent(acts.at[0, pl.ds(0, span), pl.ds(0, cols)], pair_send.at[ph, d - 1])

    def plane_sent():
        if group > 1:
            all_sent(weights.at[:, :, pl.ds(0, (group - 1) * krows), :], plane_send)

    def some_rows(i, pieces):
        l, m = chunks[i]
        return weights.at[l, m, pl.ds(0, pieces * krows), :]

    def line_sent(batch):
        l, m = chunks[batch[0]]
        ref = weights.at[l, pl.ds(m, len(batch)), pl.ds(0, block), :]

        def step(zz, carry):
            for up in (True, False):
                @pl.when(goes(batch[0], zz, up) & ((zz <= z) if up else (zz >= z)))
                def _():
                    all_sent(ref, line_send.at[0 if up else 1, share(batch[0]), zz])

            return carry

        lax.fori_loop(0, line, step, 0)

    def early_sent():
        plane_sent()
        gather_sent(0)
        gather_sent(1)
        line_sent(range(3))
        line_sent(range(3, 4))

        @functools.partial(only, host)
        def _():
            gather_sent(guests)
            all_sent(gsend, gate_send)
            for i in rest:
                all_sent(some_rows(i, group), raw_send.at[i])

        @functools.partial(only, end)
        def _():
            all_sent(acts.at[0, pl.ds(0, rows), pl.ds(0, cols)], tok_send)
            for i in rest:
                if group > 1:
                    all_sent(some_rows(i, group - 1), guest_send.at[i])

    def token_copy(p):
        return remote(own_piece(0, p), piece(2 * depth, t, q, p), tok_send, tok_recv.at[p], (partner, t))

    def gate_copy(p):
        return remote(gsend.at[pl.ds(pl.multiple_of(p * tile, tile), tile), :], piece(1, t, q, p),
                      gate_send, gate_recv.at[p], (partner, t))

    def at_tile(p):
        return pl.ds(pl.multiple_of(p * tile, tile), tile)

    def normalize(slot, l, p):
        sub = min(128, tile)

        def step(i, carry):
            at = pl.ds(pl.multiple_of(p * tile + i * sub, sub), sub)
            x = acts[slot, at, :].astype(F32)
            scale = lax.rsqrt(jnp.mean(x * x, axis=-1, keepdims=True) + 1e-06)
            normed[slot // guest, at, :] = (x * scale * gain[pl.ds(l, 1), :]).astype(BF16)
            return carry

        lax.fori_loop(0, tile // sub, step, 0)

    def project(slot, l, m, p):
        return jnp.dot(normed[slot // guest, at_tile(p), :], weights[l, m], preferred_element_type=F32).astype(BF16)

    def halo_copy(l):
        return remote(product.at[l, PIECES - 1, group - 1, pl.ds(part, 8), :], product.at[l, 0, 0, pl.ds(0, 8), :],
                      halo_send.at[l], halo_recv.at[l], (sp + group, t))

    def do_cgate(slot, l, p):
        cgate[at_tile(p), :] = project(slot, l, 0, p)

    def do_values(slot, l, p):
        values = project(slot, l, 1, p)
        made = cgate[at_tile(p), :].astype(F32) * values.astype(F32)
        for qq in range(group):
            rows_of = made[qq * part:(qq + 1) * part]
            product[slot, p, qq, pl.ds(8, part), :] = rows_of

            @pl.when(p < PIECES - 1)
            def _():
                product[slot, (p + 1) % PIECES, qq, pl.ds(0, 8), :] = rows_of[part - 8:]

            if qq + 1 < group:
                @pl.when(p == PIECES - 1)
                def _():
                    product[slot, 0, qq + 1, pl.ds(0, 8), :] = rows_of[part - 8:]

    def do_bgate(slot, l, p):
        tap = [taps[k, pl.ds(l, 1), pl.ds(own, width)] for k in range(3)]
        bgate = project(slot, l, 2, p).astype(F32)
        gated = []
        for qq in range(group):
            near = product[slot, p, qq]
            mixed = tap[0] * near[6:6 + part] + tap[1] * near[7:7 + part] + tap[2] * near[8:8 + part]
            gated.append((bgate[qq * part:(qq + 1) * part] * mixed).astype(BF16))
        return jnp.concatenate(gated, axis=0)

    def no_halo(slot):
        product[slot, 0, 0, pl.ds(0, 8), :] = jnp.zeros((8, width), F32)

    def halo_sender(l):
        return (z >= 1) & (z < line - 2) if lend and l == 0 else z < line - 1

    def halo_taker(l):
        return (z >= 2) & (z < line - 1) if lend and l == 0 else z > 0

    def halo_start(l):
        @pl.when(halo_sender(l))
        def _():
            halo_copy(l).start()

    def halo_ready(l):
        @pl.when(halo_taker(l))
        def _():
            halo_copy(l).wait_recv()

        @pl.when(z == 0)
        def _():
            no_halo(l)

    def do_out(l, p):
        update = jnp.dot(gates[l, at_tile(p), :], weights[l, 3], preferred_element_type=F32)
        return (acts[l, at_tile(p), pl.ds(own, width)].astype(F32) + update).astype(BF16)

    def out_copy(p, d):
        owner = (q + d) % group
        return remote(result.at[pl.ds(pl.multiple_of(p * tile + owner * part, part), part), :],
                      landed.at[pl.ds(pl.multiple_of(p * part, part), part),
                                pl.ds(pl.multiple_of(q * width, width), width)],
                      out_send, out_recv, in_plane(d))

    def own_gate(l, p):
        gates[l, at_tile(p), pl.ds(own, width)] = do_bgate(l, l, p)
        gather_start(2 * l + 1, p)

    guests = 2 * depth
    own_tokens = pltpu.make_async_copy(tok, acts.at[0, pl.ds(0, rows), pl.ds(0, cols)], loc_sem.at[last])
    each(lambda p: pltpu.make_async_copy(own_piece(0, p), piece(0, t, q, p), loc_sem.at[last]).start())

    @functools.partial(only, end)
    def _():
        each(lambda p: token_copy(p).start())

    rest = range(3, last)

    @functools.partial(only, end)
    def _():
        for i in range(last):
            plane_start(i)
        each(lambda p: gather_start(0, p))
        for i in range(last):
            line_start(i)
            if i in rest:
                raw_take(i)
        own_tokens.wait()
        each(lambda p: gather_relay(0, p))
        gather_all(0)

    @unless_end
    def _():
        for i in range(3):
            plane_start(i)

        @functools.partial(only, host)
        def _():
            for i in rest:
                for d in range(group):
                    raw_copy(i, d).start()

        line_start(0)

        @functools.partial(only, host)
        def _():
            def take(p):
                token_copy(p).wait_recv()
                gather_start(guests, p)
            each(take)

        line_start(1)
        line_start(2)

        @functools.partial(only, host)
        def _():
            gather_relay(guests, 0)
            gather_relay(guests, 1)

        inward(0)

        @functools.partial(only, host)
        def _():
            gather_relay(guests, 2)
            gather_relay(guests, 3)

        each(lambda p: gather_start(0, p))
        plane_start(3)
        inward(1)
        own_tokens.wait()

        @functools.partial(only, host)
        def _():
            each(lambda p: gather_last(guests, p))

            def warm(p):
                gather_paired(guests, p)
                normalize(guest, 0, p)
            each(warm)

        inward(2)
        outward(0)

        @functools.partial(only, host)
        def _():
            each(lambda p: do_cgate(guest, 0, p))

        outward(1)

        @functools.partial(only, host)
        def _():
            each(lambda p: do_values(guest, 0, p))

        each(lambda p: gather_relay(0, p))
        plane_start(4)
        plane_start(5)
        inward(3)
        outward(2)

        def lend_gate(p):
            gsend[at_tile(p), :] = do_bgate(guest, 0, p)
            gate_copy(p).start()

        @functools.partial(only, host)
        def _():
            lax.fori_loop(1, PIECES, lambda p, c: (lend_gate(p), c)[1], 0)

        line_start(3)
        inward(4)
        gather_last(0, 0)

        def take(p):
            @pl.when(p < PIECES - 1)
            def _():
                gather_last(0, p + 1)

            gather_paired(0, p)
            normalize(0, 0, p)
            do_cgate(0, 0, p)
            do_values(0, 0, p)

            @pl.when(p > 0)
            def _():
                own_gate(0, p)
        each(take)
        halo_start(0)

        @functools.partial(only, host)
        def _():
            @pl.when(z == 1)
            def _():
                no_halo(guest)
                product[0, 0, 0, pl.ds(0, 8), :] = product[guest, PIECES - 1, group - 1, pl.ds(part, 8), :]

            @pl.when(z != 1)
            def _():
                product[guest, 0, 0, pl.ds(0, 8), :] = product[0, PIECES - 1, group - 1, pl.ds(part, 8), :]

            lend_gate(0)

        halo_ready(0)
        own_gate(0, 0)
        line_start(4)
        inward(5)
        for i in range(6, last):
            plane_start(i)
        outward(3)
        line_start(5)
        gather_relay(1, 1)
        for i in range(6, last):
            inward(i)
            line_start(i)

    @functools.partial(only, end)
    def _():
        def take(p):
            gate_copy(p).wait_recv()
            gather_start(1, p)
        take(1)
        take(2)
        gather_relay(1, 1)
        take(3)
        gather_relay(1, 2)
        gather_relay(1, 3)
        take(0)
        outward(3)

    for l in range(depth):
        ph = 2 * l + 1
        if l + 1 < depth:
            def relay_next(k, p):
                on = k < PIECES - 1
                if l == 0 and lend:
                    on = on & (jnp.logical_not(end) | (k == PIECES - 2))

                @pl.when(on)
                def _():
                    gather_relay(ph, (p + 1) % PIECES)

            if l > 0:
                gather_relay(ph, 1)

            def forward(k):
                p = (k + 1) % PIECES

                @unless_end
                def _():
                    for n in range(2):
                        @pl.when(k == 2 * n)
                        def _():
                            outward(4 * l + 4 + n)
                relay_next(k, p)

                gather_finish(ph, p)
                acts[l + 1, at_tile(p), pl.ds(own, width)] = do_out(l, p)
                gather_start(ph + 1, p)
            each(forward)
            @unless_end
            def _():
                outward(4 * l + 6)
            each(lambda k: gather_relay(ph + 1, (k + 1) % PIECES))

            @functools.partial(only, end)
            def _():
                outward(4 * l + 4)
                outward(4 * l + 5)

            early_sent()

            def enter(p):
                gather_paired(ph + 1, p)
                normalize(l + 1, l + 1, p)
                do_cgate(l + 1, l + 1, p)
                do_values(l + 1, l + 1, p)

            gather_last(ph + 1, 1)
            gather_last(ph + 1, 2)
            enter(1)
            gather_last(ph + 1, 3)
            enter(2)

            unless_end(lambda: own_gate(l + 1, 2))
            gather_last(ph + 1, 0)
            enter(3)
            halo_start(l + 1)

            @functools.partial(only, end)
            def _():
                outward(4 * l + 6)
                own_gate(l + 1, 2)
            own_gate(l + 1, 3)

            @unless_end
            def _():
                outward(4 * l + 7)
            enter(0)
            own_gate(l + 1, 1)
            halo_ready(l + 1)
            own_gate(l + 1, 0)
            gather_relay(ph + 2, 2)

            @functools.partial(only, end)
            def _():
                outward(4 * l + 7)
        else:
            def finish(k):
                p = jnp.where(k < 2, k + 2, 3 - k)

                @pl.when(k < PIECES - 1)
                def _():
                    gather_relay(ph, jnp.where(k < 1, 3, 2 - k))

                gather_finish(ph, p)
                result[at_tile(p), :] = do_out(l, p)
                for d in range(1, group):
                    out_copy(p, d).start()
                landed[pl.ds(pl.multiple_of(p * part, part), part), pl.ds(pl.multiple_of(q * width, width), width)] = result[
                    pl.ds(pl.multiple_of(p * tile + q * part, part), part), :]
            each(finish)

    if group > 1:
        ref = landed.at[:, pl.ds(0, (group - 1) * width)]
        remote(ref, ref, out_send, out_recv, in_plane(1)).wait_recv()
    out[...] = landed[...]

    for l in range(1, depth):
        line_sent(range(4 * l, 4 * l + 4))
    for ph in range(2, 2 * depth):
        gather_sent(ph)

    for l in range(depth):
        @pl.when(halo_sender(l))
        def _():
            halo_copy(l).wait_send()

    if group > 1:
        all_sent(result.at[pl.ds(0, (group - 1) * rows), :], out_send)


def shards(sp_size, tps, tokens, norm_gain, w_bgate, w_cgate, w_value, conv_taps, w_out):
    rows, cols = tokens.shape
    depth, krows, _ = w_bgate.shape
    group = 4
    while group > 1 and (sp_size % group or cols % (group * LANES)):
        group //= 2
    line = sp_size // group
    width = cols // group
    span = rows * group
    full = krows * sp_size
    n = 4 * depth
    phases = 2 * depth + 1
    others = max(1, tps - 1)
    dims = (depth, group, line, tps, rows, cols, width, krows)
    anywhere = pl.BlockSpec(memory_space=pl.ANY)
    vmem = pl.BlockSpec(memory_space=pltpu.VMEM)
    dma = pltpu.SemaphoreType.DMA
    return pl.pallas_call(
        functools.partial(mixer_kernel, dims),
        out_shape=jax.ShapeDtypeStruct((rows, cols), BF16),
        in_specs=[anywhere, vmem, anywhere, anywhere, anywhere, vmem, anywhere],
        out_specs=vmem,
        scratch_shapes=[
            pltpu.VMEM((depth + 1, span, full), BF16),
            pltpu.VMEM((depth, span, full), BF16),
            pltpu.VMEM((2, span, full), BF16),
            pltpu.VMEM((depth, 4, full, width), BF16),
            pltpu.VMEM((depth + 1, PIECES, group, rows // PIECES + 8, width), F32),
            pltpu.VMEM((span, width), BF16),
            pltpu.VMEM((span, width), BF16),
            pltpu.VMEM((span, width), BF16),
            pltpu.VMEM((rows, cols), BF16),
            dma((n + 1,)), dma(()), dma((n,)),
            dma((2, depth + 1, line)), dma((n, line)),
            dma((phases,)), dma((phases, 3, PIECES)),
            dma((phases, others)), dma((phases, PIECES, others)),
            dma((depth,)), dma((depth,)), dma(()), dma(()),
            dma(()), dma((PIECES,)), dma(()), dma((PIECES,)),
            pltpu.VMEM((n, max(1, group - 1), krows, width), BF16),
            dma((n,)), dma((n,)), dma((n,)), dma((n,)),
        ],
        compiler_params=pltpu.CompilerParams(
            collective_id=0, has_side_effects=True, vmem_limit_bytes=60 * 1024 * 1024),
    )(tokens, norm_gain, w_bgate, w_cgate, w_value, conv_taps.transpose(1, 0, 2), w_out)


def solution(mesh):
    return jax.shard_map(
        functools.partial(shards, mesh.shape["sp"], mesh.shape["tp"]),
        mesh=mesh,
        in_specs=(
            P("sp", "tp"),
            P(),
            P(None, "sp", "tp"),
            P(None, "sp", "tp"),
            P(None, "sp", "tp"),
            P(),
            P(None, "sp", "tp"),
        ),
        out_specs=P("sp", "tp"),
        check_vma=False,
    )
```

```python
import functools

import jax
import jax.numpy as jnp
from jax import lax
from jax.experimental import pallas as pl
from jax.experimental.pallas import tpu as pltpu
from jax.sharding import PartitionSpec as P

MESH = pl.DeviceIdType.MESH
LANES = 128
PIECES = 4
F32 = jnp.float32
BF16 = jnp.bfloat16


def mixer_kernel(dims, tok, gain, wb, wc, wv, taps, wo, out,
                 acts, gates, normed, weights, product, cgate, gsend, result, landed,
                 loc_sem, plane_send, plane_recv, line_send, line_recv,
                 ag_send, ag_recv, pair_send, pair_recv,
                 halo_send, halo_recv, out_send, out_recv,
                 tok_send, tok_recv, gate_send, gate_recv,
                 raw, raw_send, raw_recv, guest_send, guest_recv):
    depth, group, line, tps, rows, cols, width, krows = dims
    span = rows * group
    block = krows * group
    tile = span // PIECES
    part = rows // PIECES
    lend = line >= 4
    guest = depth
    chunks = [(l, m) for l in range(depth) for m in range(4)]
    last = len(chunks)
    sources = (wc, wv, wb, wo)
    sp, t = lax.axis_index("sp"), lax.axis_index("tp")
    z, q = sp // group, sp % group
    own = pl.multiple_of(t * cols + q * width, width)
    end = (z == 0) | (z == line - 1)
    host = (z == 1) | (z == line - 2)
    partner = jnp.where((z == 0) | (z == line - 2), sp + group, sp - group)

    def only(cond, body):
        if lend:
            pl.when(cond)(body)

    def unless_end(body):
        if lend:
            pl.when(jnp.logical_not(end))(body)
        else:
            body()

    def in_plane(d):
        return (z * group + (q + d) % group, t)

    def in_pair(d):
        return (sp, (t + d) % tps)

    def remote(src, dst, send, recv, device):
        return pltpu.make_async_remote_copy(src_ref=src, dst_ref=dst, send_sem=send, recv_sem=recv,
                                            device_id=device, device_id_type=MESH)

    def each(body):
        def step(p, carry):
            body(p)
            return carry

        lax.fori_loop(0, PIECES, step, 0)

    barrier = pltpu.get_barrier_semaphore()

    def hello(device):
        pl.semaphore_signal(barrier, inc=1, device_id=device, device_id_type=MESH)

    for d in range(1, group):
        hello(in_plane(d))
    for d in range(1, tps):
        hello(in_pair(d))

    @pl.when(z > 0)
    def _():
        hello((sp - group, t))

    @pl.when(z < line - 1)
    def _():
        hello((sp + group, t))

    pl.semaphore_wait(barrier, group - 1 + tps - 1
                      + jnp.where(z > 0, 1, 0) + jnp.where(z < line - 1, 1, 0))

    def weight_rows(i, zz, qq):
        l, m = chunks[i]
        return weights.at[l, m, pl.ds(pl.multiple_of((zz * group + qq) * krows, krows), krows), :]

    def weight_block(i, zz):
        l, m = chunks[i]
        return weights.at[l, m, pl.ds(pl.multiple_of(zz * block, block), block), :]

    def weight_source(i, qq):
        l, m = chunks[i]
        return sources[m].at[l, :, pl.ds(pl.multiple_of(qq * width, width), width)]

    def plane_copy(i, d, sender):
        return remote(weight_source(i, (q + d) % group), weight_rows(i, z, sender),
                      plane_send, plane_recv.at[i], in_plane(d))

    def local_copy(i):
        return pltpu.make_async_copy(weight_source(i, q), weight_rows(i, z, q), loc_sem.at[i])

    low = 2 * z < line

    def share(i):
        l, m = chunks[i]
        return l if l == 0 and m < 3 else l + 1 if l else 1

    def line_copy(i, zz, up):
        blk = weight_block(i, zz)
        return remote(blk, blk, line_send.at[jnp.where(up, 0, 1), share(i), zz], line_recv.at[i, zz],
                      (jnp.where(up, sp + group, sp - group), t))

    def lent(i):
        l, m = chunks[i]
        return lend and l == 0 and m < 3

    def reach(i):
        return (1, line - 2) if lent(i) else (0, line - 1)

    def goes(i, zz, up):
        lo, hi = reach(i)
        on = jnp.where(up, z < hi, z > lo)
        if lend and not lent(i):
            on = on & jnp.logical_not((zz == z) & (jnp.where(up, z, line - 1 - z) == line - 2))
        return on

    def plane_start(i):
        local_copy(i).start()
        for d in range(1, group):
            plane_copy(i, d, q).start()

    def line_start(i):
        local_copy(i).wait()
        if group > 1:
            ref = some_rows(i, group - 1)
            remote(ref, ref, plane_send, plane_recv.at[i], in_plane(1)).wait_recv()
        for up in (low, jnp.logical_not(low)):
            @pl.when(goes(i, z, up))
            def _():
                line_copy(i, z, up).start()

    def line_pass(i, up, js=None):
        lo, hi = reach(i)
        j0, j1 = js or (0, line - 1)

        def step(j, carry):
            zz = jnp.where(up, z - 1 - j, z + 1 + j)
            here = (zz >= 0) & (zz < line) & (z >= lo) & (z <= hi)
            if lend and not lent(i):
                here = here & jnp.logical_not(end & (zz == jnp.where(z == 0, 1, line - 2)))

            @pl.when(here)
            def _():
                line_copy(i, zz, up).wait_recv()

                @pl.when(goes(i, zz, up))
                def _():
                    line_copy(i, zz, up).start()

            return carry

        lax.fori_loop(j0, j1, step, 0)

    def inward(i):
        line_pass(i, low)

    def outward(i, js=None):
        line_pass(i, jnp.logical_not(low), js)
        if js is None and lend and not lent(i):
            @functools.partial(only, end)
            def _():
                if group > 1:
                    ref = some_rows(i, group - 1)
                    remote(ref, ref, guest_send.at[i], guest_recv.at[i], in_plane(1)).wait_recv()

    def raw_copy(i, d):
        dst = weight_rows(i, z, q) if d == 0 else raw.at[i, d - 1]
        return remote(weight_source(i, (q + d) % group), dst, raw_send.at[i], raw_recv.at[i], (partner, t))

    def host_z():
        return jnp.where(z == 0, 1, line - 2)

    def guest_copy(i, d, sender):
        return remote(raw.at[i, d - 1], weight_rows(i, host_z(), sender),
                      guest_send.at[i], guest_recv.at[i], in_plane(d))

    def raw_take(i):
        ref = some_rows(i, group)
        remote(ref, ref, raw_send.at[i], raw_recv.at[i], (partner, t)).wait_recv()
        for d in range(1, group):
            guest_copy(i, d, q).start()

    by_rows = (0, 2 * depth)

    def piece(ph, tt, qq, p, sub=None):
        if ph in by_rows:
            size, slot, at = part, 0 if ph == 0 else guest, p * tile + qq * part
            col, wide, buf = tt * cols, cols, acts
        else:
            size, slot, at = tile, ph // 2, p * tile
            col, wide, buf = tt * cols + qq * width, width, acts if ph % 2 == 0 else gates
        if sub is not None:
            size = size // 2
            at = at + sub * size
        return buf.at[slot, pl.ds(pl.multiple_of(at, size), size), pl.ds(pl.multiple_of(col, wide), wide)]

    def own_piece(ph, p):
        if ph == 0:
            return tok.at[pl.ds(pl.multiple_of(p * part, part), part), :]
        return piece(ph, t, q, p)

    def flip(qq, bits):
        if bits & 1:
            qq = qq + 1 - 2 * (qq % 2)
        if bits & 2:
            qq = qq + 2 - 4 * ((qq // 2) % 2)
        return qq

    directs = ([1] if group >= 2 else []) + ([2] if group >= 4 else [])
    relays = [(1, 0, 2), (2, 1, 1)] if group >= 4 else []

    def direct_copy(ph, bits, p, sending):
        return remote(own_piece(ph, p), piece(ph, t, q if sending else flip(q, bits), p),
                      ag_send.at[ph], ag_recv.at[ph, bits - 1, p], (z * group + flip(q, bits), t))

    def relay_copy(ph, origin, sub, to, p, sending):
        ref = piece(ph, t, flip(q, origin if sending else 3), p, sub)
        return remote(ref, ref, ag_send.at[ph], ag_recv.at[ph, 2, p],
                      (z * group + flip(q, to), t))

    def pair_copy(ph, bits, p, d, tt):
        qq = flip(q, bits)
        src = own_piece(ph, p) if bits == 0 else piece(ph, t, qq, p)
        return remote(src, piece(ph, tt, qq, p), pair_send.at[ph, d - 1],
                      pair_recv.at[ph, p, d - 1], in_pair(d))

    def pair_start(ph, bits, p):
        for d in range(1, tps):
            pair_copy(ph, bits, p, d, t).start()

    def gather_start(ph, p):
        for bits in directs:
            direct_copy(ph, bits, p, True).start()
        pair_start(ph, 0, p)

    def gather_relay(ph, p):
        for bits in directs:
            direct_copy(ph, bits, p, False).wait_recv()
            for origin, sub, to in relays:
                if origin == bits:
                    relay_copy(ph, origin, sub, to, p, True).start()
            pair_start(ph, bits, p)

    def gather_last(ph, p):
        if relays:
            ref = piece(ph, t, flip(q, 3), p)
            remote(ref, ref, ag_send.at[ph], ag_recv.at[ph, 2, p], in_plane(1)).wait_recv()
            pair_start(ph, 3, p)

    def gather_finish(ph, p):
        gather_last(ph, p)
        gather_paired(ph, p)

    def gather_all(ph):
        each(lambda p: gather_last(ph, p))
        each(lambda p: gather_paired(ph, p))

    def gather_paired(ph, p):
        for d in range(1, tps):
            if ph in by_rows:
                ref = acts.at[0, pl.ds(0, span // PIECES), pl.ds(0, cols)]
            else:
                ref = acts.at[0, pl.ds(0, tile), pl.ds(0, cols)]
            remote(ref, ref, pair_send.at[ph, d - 1], pair_recv.at[ph, p, d - 1], in_pair(d)).wait_recv()

    def all_sent(ref, sem):
        remote(ref, ref, sem, sem, in_pair(1)).wait_send()

    def gather_sent(ph):
        k = len(directs) + len(relays) // 2
        if k:
            all_sent(acts.at[0, pl.ds(0, k * rows), pl.ds(0, cols)] if ph in by_rows
                     else acts.at[0, pl.ds(0, span), pl.ds(0, k * width)], ag_send.at[ph])
        for d in range(1, tps):
            all_sent(acts.at[0, pl.ds(0, span), pl.ds(0, cols)], pair_send.at[ph, d - 1])

    def plane_sent():
        if group > 1:
            all_sent(weights.at[:, :, pl.ds(0, (group - 1) * krows), :], plane_send)

    def some_rows(i, pieces):
        l, m = chunks[i]
        return weights.at[l, m, pl.ds(0, pieces * krows), :]

    def line_sent(batch):
        l, m = chunks[batch[0]]
        ref = weights.at[l, pl.ds(m, len(batch)), pl.ds(0, block), :]

        def step(zz, carry):
            for up in (True, False):
                @pl.when(goes(batch[0], zz, up) & ((zz <= z) if up else (zz >= z)))
                def _():
                    all_sent(ref, line_send.at[0 if up else 1, share(batch[0]), zz])

            return carry

        lax.fori_loop(0, line, step, 0)

    def early_sent():
        plane_sent()
        gather_sent(0)
        gather_sent(1)
        line_sent(range(3))
        line_sent(range(3, 4))

        @functools.partial(only, host)
        def _():
            gather_sent(guests)
            all_sent(gsend, gate_send)
            for i in rest:
                all_sent(some_rows(i, group), raw_send.at[i])

        @functools.partial(only, end)
        def _():
            all_sent(acts.at[0, pl.ds(0, rows), pl.ds(0, cols)], tok_send)
            for i in rest:
                if group > 1:
                    all_sent(some_rows(i, group - 1), guest_send.at[i])

    def token_copy(p):
        return remote(own_piece(0, p), piece(2 * depth, t, q, p), tok_send, tok_recv.at[p], (partner, t))

    def gate_copy(p):
        return remote(gsend.at[pl.ds(pl.multiple_of(p * tile, tile), tile), :], piece(1, t, q, p),
                      gate_send, gate_recv.at[p], (partner, t))

    def at_tile(p):
        return pl.ds(pl.multiple_of(p * tile, tile), tile)

    def normalize(slot, l, p):
        sub = min(128, tile)

        def step(i, carry):
            at = pl.ds(pl.multiple_of(p * tile + i * sub, sub), sub)
            x = acts[slot, at, :].astype(F32)
            scale = lax.rsqrt(jnp.mean(x * x, axis=-1, keepdims=True) + 1e-06)
            normed[slot // guest, at, :] = (x * scale * gain[pl.ds(l, 1), :]).astype(BF16)
            return carry

        lax.fori_loop(0, tile // sub, step, 0)

    def project(slot, l, m, p):
        return jnp.dot(normed[slot // guest, at_tile(p), :], weights[l, m], preferred_element_type=F32).astype(BF16)

    def halo_copy(l):
        return remote(product.at[l, PIECES - 1, group - 1, pl.ds(part, 8), :], product.at[l, 0, 0, pl.ds(0, 8), :],
                      halo_send.at[l], halo_recv.at[l], (sp + group, t))

    def do_cgate(slot, l, p):
        cgate[at_tile(p), :] = project(slot, l, 0, p)

    def do_values(slot, l, p):
        values = project(slot, l, 1, p)
        made = cgate[at_tile(p), :].astype(F32) * values.astype(F32)
        for qq in range(group):
            rows_of = made[qq * part:(qq + 1) * part]
            product[slot, p, qq, pl.ds(8, part), :] = rows_of

            @pl.when(p < PIECES - 1)
            def _():
                product[slot, (p + 1) % PIECES, qq, pl.ds(0, 8), :] = rows_of[part - 8:]

            if qq + 1 < group:
                @pl.when(p == PIECES - 1)
                def _():
                    product[slot, 0, qq + 1, pl.ds(0, 8), :] = rows_of[part - 8:]

    def do_bgate(slot, l, p):
        tap = [taps[k, pl.ds(l, 1), pl.ds(own, width)] for k in range(3)]
        bgate = project(slot, l, 2, p).astype(F32)
        gated = []
        for qq in range(group):
            near = product[slot, p, qq]
            mixed = tap[0] * near[6:6 + part] + tap[1] * near[7:7 + part] + tap[2] * near[8:8 + part]
            gated.append((bgate[qq * part:(qq + 1) * part] * mixed).astype(BF16))
        return jnp.concatenate(gated, axis=0)

    def no_halo(slot):
        product[slot, 0, 0, pl.ds(0, 8), :] = jnp.zeros((8, width), F32)

    def halo_sender(l):
        return (z >= 1) & (z < line - 2) if lend and l == 0 else z < line - 1

    def halo_taker(l):
        return (z >= 2) & (z < line - 1) if lend and l == 0 else z > 0

    def halo_start(l):
        @pl.when(halo_sender(l))
        def _():
            halo_copy(l).start()

    def halo_ready(l):
        @pl.when(halo_taker(l))
        def _():
            halo_copy(l).wait_recv()

        @pl.when(z == 0)
        def _():
            no_halo(l)

    def do_out(l, p):
        update = jnp.dot(gates[l, at_tile(p), :], weights[l, 3], preferred_element_type=F32)
        return (acts[l, at_tile(p), pl.ds(own, width)].astype(F32) + update).astype(BF16)

    def out_copy(p, d):
        owner = (q + d) % group
        return remote(result.at[pl.ds(pl.multiple_of(p * tile + owner * part, part), part), :],
                      landed.at[pl.ds(pl.multiple_of(p * part, part), part),
                                pl.ds(pl.multiple_of(q * width, width), width)],
                      out_send, out_recv, in_plane(d))

    def own_gate(l, p):
        gates[l, at_tile(p), pl.ds(own, width)] = do_bgate(l, l, p)
        gather_start(2 * l + 1, p)

    guests = 2 * depth
    own_tokens = pltpu.make_async_copy(tok, acts.at[0, pl.ds(0, rows), pl.ds(0, cols)], loc_sem.at[last])
    each(lambda p: pltpu.make_async_copy(own_piece(0, p), piece(0, t, q, p), loc_sem.at[last]).start())

    @functools.partial(only, end)
    def _():
        each(lambda p: token_copy(p).start())

    rest = range(3, last)

    @functools.partial(only, end)
    def _():
        for i in range(last):
            plane_start(i)
        each(lambda p: gather_start(0, p))
        for i in range(last):
            line_start(i)
            if i in rest:
                raw_take(i)
        own_tokens.wait()
        each(lambda p: gather_relay(0, p))
        gather_all(0)

    @unless_end
    def _():
        for i in range(3):
            plane_start(i)

        @functools.partial(only, host)
        def _():
            for i in rest:
                for d in range(group):
                    raw_copy(i, d).start()

        line_start(0)

        @functools.partial(only, host)
        def _():
            def take(p):
                token_copy(p).wait_recv()
                gather_start(guests, p)
            each(take)

        line_start(1)
        line_start(2)

        @functools.partial(only, host)
        def _():
            gather_relay(guests, 0)
            gather_relay(guests, 1)

        inward(0)

        @functools.partial(only, host)
        def _():
            gather_relay(guests, 2)
            gather_relay(guests, 3)

        each(lambda p: gather_start(0, p))
        plane_start(3)
        inward(1)
        own_tokens.wait()

        @functools.partial(only, host)
        def _():
            each(lambda p: gather_last(guests, p))

            def warm(p):
                gather_paired(guests, p)
                normalize(guest, 0, p)
            each(warm)

        inward(2)
        outward(0)

        @functools.partial(only, host)
        def _():
            each(lambda p: do_cgate(guest, 0, p))

        outward(1)

        @functools.partial(only, host)
        def _():
            each(lambda p: do_values(guest, 0, p))

        each(lambda p: gather_relay(0, p))
        plane_start(4)
        plane_start(5)
        inward(3)
        outward(2)

        def lend_gate(p):
            gsend[at_tile(p), :] = do_bgate(guest, 0, p)
            gate_copy(p).start()

        @functools.partial(only, host)
        def _():
            lax.fori_loop(1, PIECES, lambda p, c: (lend_gate(p), c)[1], 0)

        line_start(3)
        inward(4)
        gather_last(0, 0)

        def take(p):
            @pl.when(p < PIECES - 1)
            def _():
                gather_last(0, p + 1)

            gather_paired(0, p)
            normalize(0, 0, p)
            do_cgate(0, 0, p)
            do_values(0, 0, p)

            @pl.when(p > 0)
            def _():
                own_gate(0, p)
        each(take)
        halo_start(0)

        @functools.partial(only, host)
        def _():
            @pl.when(z == 1)
            def _():
                no_halo(guest)
                product[0, 0, 0, pl.ds(0, 8), :] = product[guest, PIECES - 1, group - 1, pl.ds(part, 8), :]

            @pl.when(z != 1)
            def _():
                product[guest, 0, 0, pl.ds(0, 8), :] = product[0, PIECES - 1, group - 1, pl.ds(part, 8), :]

            lend_gate(0)

        halo_ready(0)
        own_gate(0, 0)
        line_start(4)
        inward(5)
        for i in range(6, last):
            plane_start(i)
        outward(3)
        line_start(5)
        gather_relay(1, 1)
        outward(4, (0, 1))
        for i in range(6, last):
            inward(i)
            line_start(i)

    @functools.partial(only, end)
    def _():
        def take(p):
            gate_copy(p).wait_recv()
            gather_start(1, p)
        take(1)
        take(2)
        gather_relay(1, 1)
        take(3)
        gather_relay(1, 2)
        gather_relay(1, 3)
        take(0)
        outward(3)

    for l in range(depth):
        ph = 2 * l + 1
        if l + 1 < depth:
            def relay_next(k, p):
                on = k < PIECES - 1
                if l == 0 and lend:
                    on = on & (jnp.logical_not(end) | (k == PIECES - 2))

                @pl.when(on)
                def _():
                    gather_relay(ph, (p + 1) % PIECES)

            if l > 0:
                gather_relay(ph, 1)

            def forward(k):
                p = (k + 1) % PIECES

                @unless_end
                def _():
                    for n in range(2):
                        @pl.when(k == 2 * n)
                        def _():
                            outward(4 * l + 4 + n, (1, line - 1) if l + n == 0 else None)
                relay_next(k, p)

                gather_finish(ph, p)
                acts[l + 1, at_tile(p), pl.ds(own, width)] = do_out(l, p)
                gather_start(ph + 1, p)
            each(forward)
            @unless_end
            def _():
                outward(4 * l + 6)
            each(lambda k: gather_relay(ph + 1, (k + 1) % PIECES))

            @functools.partial(only, end)
            def _():
                outward(4 * l + 4)
                outward(4 * l + 5)

            early_sent()

            def enter(p):
                gather_paired(ph + 1, p)
                normalize(l + 1, l + 1, p)
                do_cgate(l + 1, l + 1, p)
                do_values(l + 1, l + 1, p)

            gather_last(ph + 1, 1)
            gather_last(ph + 1, 2)
            enter(1)
            gather_last(ph + 1, 3)
            enter(2)

            unless_end(lambda: own_gate(l + 1, 2))
            gather_last(ph + 1, 0)
            enter(3)
            halo_start(l + 1)

            @unless_end
            def _():
                own_gate(l + 1, 3)
                outward(4 * l + 7)
            enter(0)

            @functools.partial(only, end)
            def _():
                outward(4 * l + 6)
                own_gate(l + 1, 2)
                own_gate(l + 1, 3)
            own_gate(l + 1, 1)
            halo_ready(l + 1)
            own_gate(l + 1, 0)
            gather_relay(ph + 2, 2)
            gather_relay(ph + 2, 3)

            @functools.partial(only, end)
            def _():
                outward(4 * l + 7)
        else:
            def finish(k):
                p = jnp.where(k < 2, k + 2, 3 - k)

                @pl.when(k < PIECES - 2)
                def _():
                    gather_relay(ph, 1 - k)

                gather_finish(ph, p)
                result[at_tile(p), :] = do_out(l, p)
                for d in range(1, group):
                    out_copy(p, d).start()
                landed[pl.ds(pl.multiple_of(p * part, part), part), pl.ds(pl.multiple_of(q * width, width), width)] = result[
                    pl.ds(pl.multiple_of(p * tile + q * part, part), part), :]
            each(finish)

    if group > 1:
        ref = landed.at[:, pl.ds(0, (group - 1) * width)]
        remote(ref, ref, out_send, out_recv, in_plane(1)).wait_recv()
    out[...] = landed[...]

    for l in range(1, depth):
        line_sent(range(4 * l, 4 * l + 4))
    for ph in range(2, 2 * depth):
        gather_sent(ph)

    for l in range(depth):
        @pl.when(halo_sender(l))
        def _():
            halo_copy(l).wait_send()

    if group > 1:
        all_sent(result.at[pl.ds(0, (group - 1) * rows), :], out_send)


def shards(sp_size, tps, tokens, norm_gain, w_bgate, w_cgate, w_value, conv_taps, w_out):
    rows, cols = tokens.shape
    depth, krows, _ = w_bgate.shape
    group = 4
    while group > 1 and (sp_size % group or cols % (group * LANES)):
        group //= 2
    line = sp_size // group
    width = cols // group
    span = rows * group
    full = krows * sp_size
    n = 4 * depth
    phases = 2 * depth + 1
    others = max(1, tps - 1)
    dims = (depth, group, line, tps, rows, cols, width, krows)
    anywhere = pl.BlockSpec(memory_space=pl.ANY)
    vmem = pl.BlockSpec(memory_space=pltpu.VMEM)
    dma = pltpu.SemaphoreType.DMA
    return pl.pallas_call(
        functools.partial(mixer_kernel, dims),
        out_shape=jax.ShapeDtypeStruct((rows, cols), BF16),
        in_specs=[anywhere, vmem, anywhere, anywhere, anywhere, vmem, anywhere],
        out_specs=vmem,
        scratch_shapes=[
            pltpu.VMEM((depth + 1, span, full), BF16),
            pltpu.VMEM((depth, span, full), BF16),
            pltpu.VMEM((2, span, full), BF16),
            pltpu.VMEM((depth, 4, full, width), BF16),
            pltpu.VMEM((depth + 1, PIECES, group, rows // PIECES + 8, width), F32),
            pltpu.VMEM((span, width), BF16),
            pltpu.VMEM((span, width), BF16),
            pltpu.VMEM((span, width), BF16),
            pltpu.VMEM((rows, cols), BF16),
            dma((n + 1,)), dma(()), dma((n,)),
            dma((2, depth + 1, line)), dma((n, line)),
            dma((phases,)), dma((phases, 3, PIECES)),
            dma((phases, others)), dma((phases, PIECES, others)),
            dma((depth,)), dma((depth,)), dma(()), dma(()),
            dma(()), dma((PIECES,)), dma(()), dma((PIECES,)),
            pltpu.VMEM((n, max(1, group - 1), krows, width), BF16),
            dma((n,)), dma((n,)), dma((n,)), dma((n,)),
        ],
        compiler_params=pltpu.CompilerParams(
            collective_id=0, has_side_effects=True, vmem_limit_bytes=60 * 1024 * 1024),
    )(tokens, norm_gain, w_bgate, w_cgate, w_value, conv_taps.transpose(1, 0, 2), w_out)


def solution(mesh):
    return jax.shard_map(
        functools.partial(shards, mesh.shape["sp"], mesh.shape["tp"]),
        mesh=mesh,
        in_specs=(
            P("sp", "tp"),
            P(),
            P(None, "sp", "tp"),
            P(None, "sp", "tp"),
            P(None, "sp", "tp"),
            P(),
            P(None, "sp", "tp"),
        ),
        out_specs=P("sp", "tp"),
        check_vma=False,
    )
```
